256 devices in a mesh: ep: 16 (over y, x), tp: 16 (over z, core).
Axes of the slice: x: 4, y: 4, z: 8, core: 2. Of those that a mesh axis runs over, the one named last changes fastest.
Arguments:
- residual: bfloat16 [1024, 2048], P('ep'), may hold values from -20 to 20
- cache_latent: bfloat16 [1024, 2048, 256], P(('ep', 'tp')), may hold values from -12 to 12
- cache_rope: bfloat16 [1024, 32, 2048], P(('ep', 'tp')), may hold values from -6 to 6
- lengths: int32 [1024], P(('ep', 'tp')), may hold values from 2 to 2048, as said below
- query_latent: bfloat16 [1024, 32, 256], P(('ep', 'tp')), may hold values from -250 to 250
- query_rope: bfloat16 [1024, 32, 32], P(('ep', 'tp')), may hold values from -6 to 6
- norm_gain: bfloat16 [2048], replicated, may hold values from 0.099609375 to 1.8984375
- latent_weight: bfloat16 [2048, 256], replicated, may hold values from -0.125 to 0.125
- latent_gain: bfloat16 [256], replicated, may hold values from 0.099609375 to 1.8984375
- rope_weight: bfloat16 [32, 2048], replicated, may hold values from -0.125 to 0.125
- value_weight: bfloat16 [256, 2048], replicated, may hold values from -0.375 to 0.375
- out_weight: bfloat16 [2048, 2048], P('tp'), may hold values from -1 to 1
- mixer_gain: bfloat16 [2048], replicated, may hold values from 0.099609375 to 1.8984375
- group_router: bfloat16 [2048, 4], replicated, may hold values from -0.0625 to 0.0625
- expert_router: bfloat16 [2048, 32], replicated, may hold values from -0.0625 to 0.0625
- expert_ids: int32 [1024, 2], P('ep'), may hold values from 0 to 31, as said below
- gate_weight: bfloat16 [32, 2048, 4096], P('ep', None, 'tp'), may hold values from -0.125 to 0.125
- up_weight: bfloat16 [32, 2048, 4096], P('ep', None, 'tp'), may hold values from -0.125 to 0.125
- down_weight: bfloat16 [32, 4096, 2048], P('ep', 'tp'), may hold values from -0.75 to 0.75
Outputs:
- mixed: bfloat16 [1024, 2048], P('ep')
- new_latent: bfloat16 [1024, 256], P(('ep', 'tp'))
- new_rope_key: bfloat16 [1024, 32], P(('ep', 'tp'))
The draws below stay inside these ranges and needn't reach their ends.
Inputs may be any that keep to these rules, and one draw needn't show every extreme that they name: `lengths`: every sequence has 2 or more cached positions, and in every draw some sequence has all 2048. `expert_ids`: each row names 2 different experts of one group; group g holds experts g * 8 to g * 8 + 7. Among the rows of one index of ep (aligned blocks of 64 rows) no expert is named more than 8 times, and in every draw some expert is named exactly 8 times in every block.
All inputs are finite; a program needn't handle non-finite values.
Results may differ from the reference program's by a relative error of at most 0.012.
Values may be sent and summed in bfloat16 or wider, within the bound.
A program may use at most 64 MiB of HBM per device.

```python
import math
from functools import partial
import jax
import jax.numpy as jnp
from jax import lax

D = 2048
H = 32
KV = 256
ROPE = 32
NOPE = 64
V = 64
DE = 4096
GROUPS = 4
TOPK = 2
LEN = 2048
GROUP_SEQS = 64
SEQS = 1024
EXPERTS = 32
CAP = 8
N_EP = 16


def anchor_rows(key):
    base_key = jax.random.fold_in(key, 7)
    first_rows = jax.random.normal(jax.random.fold_in(base_key, 1), (SEQS, KV), jnp.float32)
    other_rows = jax.random.normal(jax.random.fold_in(base_key, 2), (SEQS, KV), jnp.float32)
    return (first_rows, other_rows)


def draw_cache_latent(key, part):
    first_rows, other_rows = anchor_rows(key)
    remaining = jax.random.normal(jax.random.fold_in(key, 3), (SEQS, LEN - 2, KV), jnp.float32)
    whole = jnp.concatenate([first_rows[:, None, :], other_rows[:, None, :], remaining], axis=1)
    return jnp.clip(whole, -12.0, 12.0).astype(jnp.bfloat16)


def draw_query_latent(key, part):
    values = jax.random.normal(jax.random.fold_in(key, 5), (SEQS, H, KV), jnp.float32)
    return jnp.clip(values, -250.0, 250.0).astype(jnp.bfloat16)


def draw_residual(key, part):
    base_key = jax.random.fold_in(key, 13)
    column_scale = jnp.exp(jax.random.uniform(jax.random.fold_in(base_key, 1), (D,), jnp.float32, math.log(0.3), math.log(3.0)))
    values = jax.random.normal(jax.random.fold_in(base_key, 2), (SEQS, D), jnp.float32)
    return jnp.clip(values * column_scale[None, :], -20.0, 20.0).astype(jnp.bfloat16)


def draw_lengths(key, part):
    base_key = jax.random.fold_in(key, 17)
    exponent = jax.random.randint(jax.random.fold_in(base_key, 1), (SEQS,), 1, 14)
    spans = jnp.left_shift(jnp.ones((SEQS,), jnp.int32), exponent.astype(jnp.int32))
    drawn = 2 + jax.random.randint(jax.random.fold_in(base_key, 2), (SEQS,), 0, spans)
    drawn = jnp.minimum(drawn, LEN)
    chosen = jax.random.randint(jax.random.fold_in(base_key, 3), (), 0, SEQS)
    return jnp.where(jnp.arange(SEQS) == chosen, LEN, drawn).astype(jnp.int32)


def draw_expert_ids(key, part):
    base_key = jax.random.fold_in(key, 19)
    per_group = EXPERTS // GROUPS
    half_rows = GROUP_SEQS // 2
    busiest = jax.random.randint(jax.random.fold_in(base_key, 1), (), 0, GROUPS).astype(jnp.int32)

    def one_block(block_key):
        others = (busiest + jax.random.randint(jax.random.fold_in(block_key, 1), (GROUP_SEQS - half_rows,), 1, GROUPS)) % GROUPS
        chosen = jnp.concatenate([jnp.full((half_rows,), busiest, jnp.int32), others.astype(jnp.int32)])
        hit_table = (chosen[:, None] == jnp.arange(GROUPS, dtype=jnp.int32)[None, :]).astype(jnp.int32)
        order_in_group = jnp.sum((jnp.cumsum(hit_table, axis=0) - hit_table) * hit_table, axis=1)
        offsets = jax.random.randint(jax.random.fold_in(block_key, 2), (GROUPS,), 0, per_group)
        orders = jax.vmap(lambda sub_key: jax.random.permutation(sub_key, per_group))(jax.random.split(jax.random.fold_in(block_key, 3), GROUPS))
        first_slot = (offsets[chosen] + 2 * order_in_group) % per_group
        second_slot = (first_slot + 1) % per_group
        first_id = chosen * per_group + orders[chosen, first_slot]
        second_id = chosen * per_group + orders[chosen, second_slot]
        paired = jnp.stack([first_id, second_id], axis=1)
        shuffle = jax.random.permutation(jax.random.fold_in(block_key, 4), GROUP_SEQS)
        return paired[shuffle]
    block_keys = jax.random.split(jax.random.fold_in(base_key, 2), SEQS // GROUP_SEQS)
    return jax.vmap(one_block)(block_keys).reshape(SEQS, TOPK).astype(jnp.int32)


def spiked(values, stream_key, source, target, blocks, factor):
    owner, partner = [(jnp.arange(values.shape[dim]) // (values.shape[dim] // blocks)).reshape([-1 if axis == dim else 1 for axis in range(values.ndim)]) for dim in (source, target)]
    chosen = jax.random.permutation(stream_key, blocks)[partner]
    strong = (owner == chosen) | (owner == (partner + blocks // 2) % blocks)
    return jnp.where(strong, factor * values, values)


def block_scale(key, shape, pieces, low, largest):
    loudness, own = 1.0, jax.random.fold_in(key, 6)
    for dim, blocks in pieces:
        draws = jnp.exp(jax.random.uniform(jax.random.fold_in(own, dim), (blocks,), jnp.float32, low / len(pieces), largest / len(pieces)))
        loudness = loudness * jnp.repeat(draws, shape[dim] // blocks).reshape([-1 if axis == dim else 1 for axis in range(len(shape))])
    return loudness


def gaussian(key, extent, scale, reach, cuts=(), kind=jnp.bfloat16):
    values = jax.random.normal(key, extent, jnp.float32) * scale
    if len(cuts) > 0:
        values = block_scale(key, extent, cuts, -0.22, 0.18) * values
    return jnp.clip(values, min=-reach, max=reach).astype(kind)


def bell_draw_with(stream_key, dims, spread, limit, cuts, heavy, held_as=jnp.bfloat16):
    result = spread * jax.random.normal(stream_key, dims, jnp.float32)
    if cuts:
        result = result * block_scale(stream_key, dims, cuts, -0.22, 0.18)
    return jnp.clip(spiked(result, jax.random.fold_in(stream_key, 3), *heavy), -limit, limit).astype(held_as)


def setup_inputs(seed: int = 0) -> dict:
    splits = jax.random.split(jax.random.key(seed), 20)
    residual = draw_residual(jax.random.fold_in(splits[19], 71), 0)
    cache_latent = draw_cache_latent(jax.random.fold_in(splits[19], 71), 0)
    cache_rope = gaussian(splits[2], (SEQS, ROPE, LEN), 1.0, 6.0, ((0, 256),))
    lengths = draw_lengths(jax.random.fold_in(splits[19], 71), 0)
    query_latent = draw_query_latent(jax.random.fold_in(splits[19], 71), 0)
    query_rope = gaussian(splits[5], (SEQS, H, ROPE), 1.0, 6.0, ((0, 256),))
    norm_gain = jnp.clip(1.0 + 0.18 * jax.random.normal(splits[6], (D,), jnp.float32), 0.099609375, 1.8984375).astype(jnp.bfloat16)
    latent_weight = gaussian(splits[7], (D, KV), D ** -0.5, 0.125)
    latent_gain = jnp.clip(1.0 + 0.18 * jax.random.normal(splits[8], (KV,), jnp.float32), 0.099609375, 1.8984375).astype(jnp.bfloat16)
    rope_weight = gaussian(splits[9], (ROPE, D), D ** -0.5, 0.125)
    value_weight = gaussian(splits[10], (KV, H * V), KV ** -0.5, 0.375)
    out_weight = bell_draw_with(splits[11], (H * V, D), (H * V // 32) ** -0.5, 1.0, ((0, 16),), (0, 1, 16, 2.0))
    mixer_gain = jnp.clip(1.0 + 0.18 * jax.random.normal(splits[12], (D,), jnp.float32), 0.099609375, 1.8984375).astype(jnp.bfloat16)
    group_router = gaussian(splits[13], (D, GROUPS), (4 * D) ** -0.5, 0.0625)
    expert_router = gaussian(splits[14], (D, EXPERTS), (4 * D) ** -0.5, 0.0625)
    expert_ids = draw_expert_ids(jax.random.fold_in(splits[19], 71), 0)
    gate_weight = gaussian(splits[16], (EXPERTS, D, DE), D ** -0.5, 0.125, ((0, 16), (2, 16)))
    up_weight = gaussian(splits[17], (EXPERTS, D, DE), D ** -0.5, 0.125, ((0, 16), (2, 16)))
    down_weight = gaussian(splits[18], (EXPERTS, DE, D), (DE // 64) ** -0.5, 0.75, ((0, 16), (1, 16)))
    return {"residual": residual, "cache_latent": cache_latent, "cache_rope": cache_rope, "lengths": lengths, "query_latent": query_latent, "query_rope": query_rope, "norm_gain": norm_gain, "latent_weight": latent_weight, "latent_gain": latent_gain, "rope_weight": rope_weight, "value_weight": value_weight, "out_weight": out_weight, "mixer_gain": mixer_gain, "group_router": group_router, "expert_router": expert_router, "expert_ids": expert_ids, "gate_weight": gate_weight, "up_weight": up_weight, "down_weight": down_weight}


NORM_EPSILON = 1e-06
ROPE_BASE = 10000.0

def inverse_rms(values):
    return lax.rsqrt(lax.optimization_barrier(jnp.mean(values * values, axis=-1, keepdims=True)) + NORM_EPSILON)

def rotate(vector, position):
    half_width = vector.shape[-1] // 2
    frequency = ROPE_BASE ** (-jnp.arange(0, vector.shape[-1], 2, dtype=jnp.float32) / vector.shape[-1])
    angles = position[..., None] * frequency
    lower_half = vector[..., :half_width]
    upper_half = vector[..., half_width:]
    return jnp.concatenate([lower_half * jnp.cos(angles) - upper_half * jnp.sin(angles), upper_half * jnp.cos(angles) + lower_half * jnp.sin(angles)], axis=-1)

def dispatch_table(expert_rows, experts, capacity):
    flat_ids = expert_rows.reshape(-1)
    hit_table = (flat_ids[:, None] == jnp.arange(experts, dtype=jnp.int32)[None, :]).astype(jnp.int32)
    slot_rank = lax.optimization_barrier(jnp.sum((jnp.cumsum(hit_table, axis=0) - hit_table) * hit_table, axis=1))
    slot_index = flat_ids * capacity + slot_rank
    picked = (slot_index[None, :] == jnp.arange(experts * capacity, dtype=jnp.int32)[:, None]).astype(jnp.float32)
    return picked.reshape(experts * capacity, expert_rows.shape[0], expert_rows.shape[1])

def route_weights(expert_in, group_router, expert_router, expert_ids, per_group):
    group_logits = jnp.dot(expert_in, group_router, preferred_element_type=jnp.float32)
    expert_logits = jnp.dot(expert_in, expert_router, preferred_element_type=jnp.float32)
    chosen = expert_ids[:, 0] // per_group
    group_hit = (jnp.arange(group_logits.shape[1], dtype=jnp.int32)[None, :] == chosen[:, None]).astype(jnp.float32)
    chosen_logit = lax.optimization_barrier(jnp.sum(group_logits * group_hit, axis=1, keepdims=True))
    group_share = 1.0 / lax.optimization_barrier(jnp.sum(jnp.exp(group_logits - chosen_logit), axis=1))
    expert_hit = (expert_ids[:, :, None] == jnp.arange(expert_logits.shape[1], dtype=jnp.int32)[None, None, :]).astype(jnp.float32)
    picked_logit = lax.optimization_barrier(jnp.sum(expert_hit * expert_logits[:, None, :], axis=2))
    inner_share = 1.0 / lax.optimization_barrier(jnp.sum(jnp.exp(picked_logit[:, None, :] - picked_logit[:, :, None]), axis=2))
    return group_share[:, None] * inner_share

def attend_one(args):
    latent_rows, rope_rows, length, query_lat, query_rot, fresh_latent, fresh_rope = args
    score_scale = (NOPE + ROPE) ** (-0.5)
    cached = (jnp.dot(query_lat, latent_rows.T, preferred_element_type=jnp.float32) + jnp.dot(query_rot, rope_rows, preferred_element_type=jnp.float32)) * score_scale
    keeping = jnp.arange(latent_rows.shape[0], dtype=jnp.int32) < length
    cached = jnp.where(keeping[None, :], cached, -jnp.inf)
    fresh = (jnp.dot(query_lat, fresh_latent, preferred_element_type=jnp.float32) + jnp.dot(query_rot, fresh_rope, preferred_element_type=jnp.float32)) * score_scale
    row_top = jnp.maximum(lax.optimization_barrier(jnp.max(cached, axis=1)), fresh)
    cached_exp = jnp.exp(cached - row_top[:, None])
    fresh_exp = jnp.exp(fresh - row_top)
    denominator = lax.optimization_barrier(jnp.sum(cached_exp, axis=1)) + fresh_exp
    cached_weight = (cached_exp / denominator[:, None]).astype(jnp.bfloat16)
    fresh_weight = (fresh_exp / denominator).astype(jnp.bfloat16)
    combined = jnp.dot(cached_weight, latent_rows, preferred_element_type=jnp.float32) + fresh_weight.astype(jnp.float32)[:, None] * fresh_latent.astype(jnp.float32)[None, :]
    return combined.astype(jnp.bfloat16)

def run_expert(args):
    rows, gate_part, up_part, down_part = args
    gate_value = jnp.dot(rows, gate_part, preferred_element_type=jnp.float32)
    up_value = jnp.dot(rows, up_part, preferred_element_type=jnp.float32)
    activation = (jax.nn.silu(gate_value) * up_value).astype(jnp.bfloat16)
    return jnp.dot(activation, down_part, preferred_element_type=jnp.float32)

def reference(residual, cache_latent, cache_rope, lengths, query_latent, query_rope, norm_gain, latent_weight, latent_gain, rope_weight, value_weight, out_weight, mixer_gain, group_router, expert_router, expert_ids, gate_weight, up_weight, down_weight):
    resid_f = residual.astype(jnp.float32)
    normed = (resid_f * inverse_rms(resid_f) * norm_gain.astype(jnp.float32)).astype(jnp.bfloat16)
    latent_raw = jnp.dot(normed, latent_weight, preferred_element_type=jnp.float32)
    new_latent = (latent_raw * inverse_rms(latent_raw) * latent_gain.astype(jnp.float32)).astype(jnp.bfloat16)
    positions = lengths.astype(jnp.float32)
    rope_raw = jnp.dot(normed, rope_weight.T, preferred_element_type=jnp.float32)
    new_rope_key = rotate(rope_raw, positions).astype(jnp.bfloat16)
    query_turned = rotate(query_rope.astype(jnp.float32), positions[:, None]).astype(jnp.bfloat16)
    mixed_latent = lax.map(attend_one, (cache_latent, cache_rope, lengths, query_latent, query_turned, new_latent, new_rope_key))
    head_values = jnp.einsum('shc,chv->shv', mixed_latent.astype(jnp.float32), value_weight.reshape(KV, H, V).astype(jnp.float32)).astype(jnp.bfloat16)
    attended = jnp.dot(head_values.reshape(SEQS, H * V), out_weight, preferred_element_type=jnp.float32)
    after_attention = (resid_f + attended).astype(jnp.bfloat16)
    after_f = after_attention.astype(jnp.float32)
    expert_in = (after_f * inverse_rms(after_f) * mixer_gain.astype(jnp.float32)).astype(jnp.bfloat16)
    route_weight = route_weights(expert_in, group_router, expert_router, expert_ids, EXPERTS // GROUPS)
    ids_blocks = expert_ids.reshape(N_EP, GROUP_SEQS, TOPK)
    picked = jax.vmap(partial(dispatch_table, experts=EXPERTS, capacity=CAP))(ids_blocks)
    select_rows = lax.optimization_barrier(jnp.sum(picked, axis=3))
    outbound = jnp.einsum('bsr,brd->bsd', select_rows, expert_in.reshape(N_EP, GROUP_SEQS, D).astype(jnp.float32), precision=lax.Precision.HIGHEST).astype(jnp.bfloat16)
    per_expert = outbound.reshape(N_EP, EXPERTS, CAP, D).transpose(1, 0, 2, 3).reshape(EXPERTS, N_EP * CAP, D)
    expert_out = lax.map(run_expert, (per_expert, gate_weight, up_weight, down_weight))
    back_blocks = expert_out.reshape(EXPERTS, N_EP, CAP, D).transpose(1, 0, 2, 3).reshape(N_EP, EXPERTS * CAP, D)
    combine = lax.optimization_barrier(jnp.sum(picked * route_weight.reshape(N_EP, 1, GROUP_SEQS, TOPK), axis=3))
    moe_sum = jnp.einsum('bsr,bsd->brd', combine, back_blocks, precision=lax.Precision.HIGHEST).reshape(SEQS, D)
    mixed = (after_f + moe_sum).astype(jnp.bfloat16)
    return (mixed, new_latent, new_rope_key)
```

```python
import functools
import math

import jax
import jax.numpy as jnp
from jax import lax
from jax.experimental import pallas as pl
from jax.experimental.pallas import tpu as pltpu
from jax.sharding import PartitionSpec as P

MESH = pl.DeviceIdType.MESH
F32 = jnp.float32
BF16 = jnp.bfloat16
I32 = jnp.int32

D = 2048
HALF = D // 2
H = 32
KV = 256
ROPE = 32
NOPE = 64
V = 64
GROUPS = 4
LEN = 2048
CAP = 8
N_EP = 16
N_TP = 16
NZ = 8
SEQS = 4
ROWS = 64
EXPERTS = 32
SLOTS = EXPERTS * CAP
SHARE = 128
HID = 256
EPS = 1e-06
ROPE_BASE = 10000.0


def dot(a, b):
    return jnp.dot(a, b, preferred_element_type=F32)


def dot_t(a, b):
    return lax.dot_general(a, b, (((1,), (1,)), ((), ())), preferred_element_type=F32)


def iota(shape, dim):
    return lax.broadcasted_iota(I32, shape, dim)


def kernel(
    residual,
    cache_latent,
    cache_rope,
    lengths,
    query_latent,
    query_rope,
    norm_gain,
    latent_weight,
    latent_gain,
    rope_weight,
    value_weight,
    out_weight,
    mixer_gain,
    group_router,
    expert_router,
    ids,
    gate_weight,
    up_weight,
    down_weight,
    mixed_out,
    new_latent_out,
    new_rope_out,
    res8,
    res_cols,
    cl,
    cr,
    ql,
    qr,
    ng,
    lw,
    lg,
    rw,
    vw,
    ow,
    mg,
    grt,
    ert,
    idv,
    gw,
    uw,
    dw,
    mixl,
    hv_send,
    hv_recv,
    acc,
    rs_send,
    rs_recv,
    after,
    after_other,
    full,
    sel,
    disp,
    xin,
    xn,
    ret,
    yin,
    comb,
    rs2_send,
    rs2_recv,
    fin,
    local_sem,
    w_ssem,
    w_rsem,
    hv_ssem,
    hv_rsem,
    rs_ssem,
    rs_rsem,
    ag_ssem,
    ag_rsem,
    ot_ssem,
    ot_rsem,
    x_ssem,
    x_rsem,
    y_ssem,
    y_rsem,
    rs2_ssem,
    rs2_rsem,
    f_ssem,
    f_rsem,
    p_ssem,
    p_rsem,
):
    ep = lax.axis_index("ep")
    tp = lax.axis_index("tp")
    z = lax.div(tp, 2)
    c = lax.rem(tp, 2)
    other = 1 - c
    partner = z * 2 + other

    def remote(src, dst, ssem, rsem, to_ep, to_tp):
        return pltpu.make_async_remote_copy(
            src_ref=src,
            dst_ref=dst,
            send_sem=ssem,
            recv_sem=rsem,
            device_id=(to_ep, to_tp),
            device_id_type=MESH,
        )

    def ring(i):
        return lax.rem(z + i, NZ)

    barrier = pltpu.get_barrier_semaphore()

    def signal_tp(i, carry):
        pl.semaphore_signal(
            barrier, inc=1, device_id=(ep, lax.rem(tp + i, N_TP)), device_id_type=MESH
        )
        return carry

    def signal_ep(i, carry):
        there = lax.rem(ep + i, N_EP)
        for core in range(2):
            pl.semaphore_signal(
                barrier, inc=1, device_id=(there, z * 2 + core), device_id_type=MESH
            )
        return carry

    lax.fori_loop(1, N_TP, signal_tp, 0)
    lax.fori_loop(1, N_EP, signal_ep, 0)

    loads = {}

    def load(name, src, dst):
        copy = pltpu.make_async_copy(src, dst, local_sem.at[len(loads)])
        copy.start()
        loads[name] = copy

    load("res8", residual.at[pl.ds(pl.multiple_of(z * 8, 8), 8), :], res8)
    load("ng", norm_gain, ng)
    load("lg", latent_gain, lg)
    load("rw", rope_weight, rw)
    load("qr", query_rope, qr)
    load("lw", latent_weight, lw)
    load("ql", query_latent, ql)
    for s in range(SEQS):
        load(f"cr{s}", cache_rope.at[s], cr.at[s])
        load(f"cl{s}", cache_latent.at[s], cl.at[s])
    load("vw", value_weight, vw)
    load("ow", out_weight.at[:, pl.ds(pl.multiple_of(c * HALF, HALF), HALF)], ow.at[c])
    share_at = pl.multiple_of(c * HALF + z * SHARE, SHARE)
    load("res_cols", residual.at[:, pl.ds(share_at, SHARE)], res_cols)
    load("ids", ids, idv)
    load("mg", mixer_gain, mg)
    load("grt", group_router, grt)
    load("ert", expert_router, ert)
    load("gw", gate_weight.at[c], gw.at[0])
    load("uw", up_weight.at[c], uw.at[0])
    load("dw", down_weight.at[c], dw.at[0])

    loads["res8"].wait()
    loads["ng"].wait()
    rows = res8[...].astype(F32)
    inv = lax.rsqrt(jnp.mean(rows * rows, axis=1, keepdims=True) + EPS)
    normed = (rows * inv * ng[...].astype(F32)).astype(BF16)
    loads["rw"].wait()
    rope_raw = dot_t(normed, rw[...])
    loads["lw"].wait()
    latent_raw = dot(normed, lw[...])
    inv = lax.rsqrt(jnp.mean(latent_raw * latent_raw, axis=1, keepdims=True) + EPS)
    loads["lg"].wait()
    latent8 = latent_raw * inv * lg[...].astype(F32)

    def own_rows(v):
        first = (iota(v.shape, 0) * 0 + c) == 0
        return jnp.where(first, v, pltpu.roll(v, 4, 0))

    new_latent = own_rows(latent8).astype(BF16)
    new_latent_out[...] = new_latent[0:SEQS]
    rope_own = own_rows(rope_raw)

    lane = iota((8, ROPE), 1)
    row = iota((8, ROPE), 0)
    place = lax.rem(lane, ROPE // 2).astype(F32)
    freq = jnp.exp(place * (-math.log(ROPE_BASE) / (ROPE // 2)))
    pos = jnp.zeros((8, ROPE), I32)
    for s in range(SEQS):
        pos = jnp.where(row == s, lengths[s], pos)
    angle = pos.astype(F32) * freq
    cos = jnp.cos(angle)
    sin = jnp.sin(angle)
    sin = jnp.where(lane < ROPE // 2, -sin, sin)

    def swapped(u):
        return jnp.concatenate([u[:, ROPE // 2 :], u[:, : ROPE // 2]], axis=1)

    new_rope = (rope_own * cos + swapped(rope_own) * sin).astype(BF16)
    new_rope_out[...] = new_rope[0:SEQS]
    new_latent_f = new_latent.astype(F32)
    new_rope_f = new_rope.astype(F32)

    scale = (NOPE + ROPE) ** (-0.5)
    loads["qr"].wait()
    loads["ql"].wait()
    for s in range(SEQS):
        u = qr[s].astype(F32)
        turned = (u * cos[s : s + 1] + swapped(u) * sin[s : s + 1]).astype(BF16)
        q = ql[s]
        loads[f"cr{s}"].wait()
        loads[f"cl{s}"].wait()
        latents = cl[s]
        score = (dot_t(q, latents) + dot(turned, cr[s])) * scale
        keep = iota((H, LEN), 1) < lengths[s]
        score = jnp.where(keep, score, -jnp.inf)
        fresh = (
            jnp.sum(q.astype(F32) * new_latent_f[s : s + 1], axis=1, keepdims=True)
            + jnp.sum(turned.astype(F32) * new_rope_f[s : s + 1], axis=1, keepdims=True)
        ) * scale
        top = jnp.maximum(jnp.max(score, axis=1, keepdims=True), fresh)
        e = jnp.exp(score - top)
        fresh_e = jnp.exp(fresh - top)
        total = jnp.sum(e, axis=1, keepdims=True) + fresh_e
        weight = (e / total).astype(BF16)
        fresh_w = (fresh_e / total).astype(BF16).astype(F32)
        mixed = dot(weight, latents) + fresh_w * new_latent_f[s : s + 1]
        mixl[s * H : (s + 1) * H, :] = mixed.astype(BF16)
        if s == 0:
            pl.semaphore_wait(barrier, 45)
            swaps = [
                remote(
                    out_weight.at[:, pl.ds(pl.multiple_of(other * HALF, HALF), HALF)],
                    ow.at[c],
                    w_ssem.at[0],
                    w_rsem.at[0],
                    ep,
                    partner,
                ),
                remote(gate_weight.at[other], gw.at[1], w_ssem.at[1], w_rsem.at[1], ep, partner),
                remote(up_weight.at[other], uw.at[1], w_ssem.at[2], w_rsem.at[2], ep, partner),
                remote(down_weight.at[other], dw.at[1], w_ssem.at[3], w_rsem.at[3], ep, partner),
            ]
            for copy in swaps:
                copy.start()

    loads["vw"].wait()
    wide = dot(mixl[...], vw[...])
    own = (iota((SEQS * H, D), 1) // V) == lax.rem(iota((SEQS * H, D), 0), H)
    wide = jnp.where(own, wide, 0.0).astype(BF16)
    pick = (iota((8, SEQS * H), 1) // H) == lax.rem(iota((8, SEQS * H), 0), SEQS)
    heads = dot(pick.astype(F32).astype(BF16), wide)
    low = iota((8, SHARE), 0) < SEQS
    for zz in range(NZ):
        a = heads[:, zz * 256 : zz * 256 + 128]
        b = heads[:, zz * 256 + 128 : zz * 256 + 256]
        hv_send[zz] = jnp.where(low, a, b).astype(BF16)

    def hv_copy(i):
        there = lax.rem(tp + i, N_TP)
        return remote(
            hv_send.at[lax.div(there, 2)], hv_recv.at[tp], hv_ssem.at[i], hv_rsem.at[tp], ep, there
        )

    def hv_start(i, carry):
        hv_copy(lax.rem(i + 7, N_TP - 1) + 1).start()
        return carry

    lax.fori_loop(0, N_TP - 1, hv_start, 0)
    hv_recv[tp] = hv_send[z]

    loads["ids"].wait()
    idr = idv[...]
    e_row = [idr[k : k + 1, :] for k in range(2)]
    eye = iota((ROWS, ROWS), 0) == iota((ROWS, ROWS), 1)

    def to_col(v):
        return jnp.sum(jnp.where(eye, jnp.broadcast_to(v, (ROWS, ROWS)), 0.0), axis=1, keepdims=True)

    def to_row(v):
        return jnp.sum(jnp.where(eye, jnp.broadcast_to(v, (ROWS, ROWS)), 0.0), axis=0, keepdims=True)

    e_col = [to_col(v.astype(F32)) for v in e_row]
    expert_iota = iota((ROWS, EXPERTS), 1).astype(F32)
    hits = [(jnp.broadcast_to(v, (ROWS, EXPERTS)) == expert_iota).astype(F32) for v in e_col]
    before = (iota((ROWS, ROWS), 1) < iota((ROWS, ROWS), 0)).astype(F32).astype(BF16)
    counts = dot(before, (hits[0] + hits[1]).astype(BF16))
    slot_col = [
        e_col[k] * CAP + jnp.sum(counts * hits[k], axis=1, keepdims=True) for k in range(2)
    ]
    slot_iota = iota((SLOTS, ROWS), 0).astype(F32)
    chosen = jnp.zeros((SLOTS, ROWS), F32)
    for k in range(2):
        chosen += (jnp.broadcast_to(to_row(slot_col[k]), (SLOTS, ROWS)) == slot_iota).astype(F32)
    sel[...] = chosen.astype(BF16)

    def hv_wait(i, carry):
        src = lax.rem(tp + i, N_TP)
        remote(
            hv_send.at[0], hv_recv.at[src], hv_ssem.at[i], hv_rsem.at[src], ep, src
        ).wait_recv()
        return carry

    lax.fori_loop(1, N_TP, hv_wait, 0)

    loads["ow"].wait()
    swaps[0].wait_recv()
    heads_in = hv_recv[...].astype(F32).reshape(N_TP * 8, SHARE).astype(BF16)
    part = None
    for k in range(2):
        r = iota((ROWS, N_TP * 8), 0)
        j = iota((ROWS, N_TP * 8), 1)
        rows_k = (j == 8 * (r // SEQS) + SEQS * k + lax.rem(r, SEQS)).astype(F32).astype(BF16)
        term = dot(dot(rows_k, heads_in).astype(BF16), ow[k])
        part = term if part is None else part + term
    for zz in range(NZ):
        piece = part[:, zz * SHARE : (zz + 1) * SHARE]
        acc[zz] = piece
        rs_send[zz] = piece.astype(BF16)

    order = (4, 3, 5, 2, 6, 1, 7)

    def scatter(send, recv, ssem, rsem):
        def copy(i):
            to = ring(i)
            return remote(
                send.at[to], recv.at[z], ssem.at[i], rsem.at[z], ep, to * 2 + c
            )

        for i in order:
            copy(i).start()

    def scatter_wait(send, recv, ssem, rsem, total):
        for i in reversed(order):
            src = ring(i)
            remote(
                send.at[src], recv.at[src], ssem.at[i], rsem.at[src], ep, src * 2 + c
            ).wait_recv()
            total += recv[src].astype(F32)
        return total

    scatter(rs_send, rs_recv, rs_ssem, rs_rsem)
    loads["res_cols"].wait()
    total = res_cols[...].astype(F32) + scatter_wait(rs_send, rs_recv, rs_ssem, rs_rsem, acc[z])
    after[z] = total.astype(BF16)

    def ag_copy(i, src):
        return remote(
            after.at[src], after.at[src], ag_ssem.at[i], ag_rsem.at[src], ep, ring(i) * 2 + c
        )

    for i in order:
        ag_copy(i, z).start()

    def place_slots(zz):
        at = pl.ds(pl.multiple_of(zz * SHARE, SHARE), SHARE)
        disp[:, at] = dot(sel[...], after[zz]).astype(BF16)

    place_slots(z)
    for i in reversed(order):
        src = ring(i)
        remote(
            after.at[z], after.at[src], ag_ssem.at[i], ag_rsem.at[src], ep, src * 2 + c
        ).wait_recv()
        place_slots(src)

    def x_copy(i, core):
        there = lax.rem(ep + i, N_EP)
        at = pl.ds(pl.multiple_of((there * 2 + core) * CAP, CAP), CAP)
        to = pl.ds(pl.multiple_of(ep * CAP, CAP), CAP)
        return remote(
            disp.at[at, :],
            xin.at[c, to, :],
            x_ssem.at[i * 2 + core],
            x_rsem.at[ep * 2 + c],
            there,
            z * 2 + core,
        )

    def x_start(i, carry):
        for core in range(2):
            x_copy(i, core).start()
        return carry

    lax.fori_loop(1, N_EP, x_start, 0)
    x_copy(0, other).start()
    mine = pl.ds(pl.multiple_of((ep * 2 + c) * CAP, CAP), CAP)
    here = pl.ds(pl.multiple_of(ep * CAP, CAP), CAP)
    xin[c, here, :] = disp[mine, :]
    to_partner = remote(after, after_other, ot_ssem, ot_rsem, ep, partner)
    to_partner.start()

    loads["mg"].wait()
    loads["grt"].wait()
    loads["ert"].wait()
    to_partner.wait_recv()
    for zz in range(NZ):
        at = pl.ds(pl.multiple_of(c * HALF + zz * SHARE, SHARE), SHARE)
        full[:, at] = after[zz]
        at = pl.ds(pl.multiple_of(other * HALF + zz * SHARE, SHARE), SHARE)
        full[:, at] = after_other[zz]
    gain = mg[...].astype(F32)
    rows = full[...].astype(F32)
    inv = lax.rsqrt(jnp.mean(rows * rows, axis=1, keepdims=True) + EPS)
    expert_in = (rows * inv * gain).astype(BF16)
    group_logits = dot_t(expert_in, grt[...])
    expert_logits = dot_t(expert_in, ert[...])
    group_of = jnp.floor(e_col[0] * (GROUPS / EXPERTS))
    group_hit = jnp.broadcast_to(group_of, (ROWS, GROUPS)) == iota((ROWS, GROUPS), 1).astype(F32)
    group_pick = jnp.sum(jnp.where(group_hit, group_logits, 0.0), axis=1, keepdims=True)
    share = 1.0 / jnp.sum(jnp.exp(group_logits - group_pick), axis=1, keepdims=True)
    picked = [jnp.sum(hits[k] * expert_logits, axis=1, keepdims=True) for k in range(2)]
    weights = jnp.zeros((ROWS, SLOTS), F32)
    wide_iota = iota((ROWS, SLOTS), 1).astype(F32)
    for k in range(2):
        inner = 1.0 / (1.0 + jnp.exp(picked[1 - k] - picked[k]))
        weights += jnp.where(
            jnp.broadcast_to(slot_col[k], (ROWS, SLOTS)) == wide_iota, share * inner, 0.0
        )
    high = weights.astype(BF16)
    comb[0:ROWS, :] = high
    comb[ROWS:, :] = (weights - high.astype(F32)).astype(BF16)

    def x_wait(i, carry):
        src = lax.rem(ep + i, N_EP)
        at = pl.ds(pl.multiple_of(src * CAP, CAP), CAP)
        for core in range(2):
            remote(
                disp.at[at, :],
                xin.at[core, at, :],
                x_ssem.at[i * 2 + core],
                x_rsem.at[src * 2 + core],
                src,
                z * 2 + core,
            ).wait_recv()
        return carry

    remote(
        disp.at[here, :],
        xin.at[other, here, :],
        x_ssem.at[other],
        x_rsem.at[ep * 2 + other],
        ep,
        partner,
    ).wait_recv()
    lax.fori_loop(1, N_EP, x_wait, 0)
    x0 = xin[0].astype(F32)
    x1 = xin[1].astype(F32)
    square = jnp.sum(x0 * x0, axis=1, keepdims=True) + jnp.sum(x1 * x1, axis=1, keepdims=True)
    inv = lax.rsqrt(square * (1.0 / D) + EPS)
    xn[:, 0:HALF] = (x0 * inv * gain[:, 0:HALF]).astype(BF16)
    xn[:, HALF:] = (x1 * inv * gain[:, HALF:]).astype(BF16)
    acts = []
    for name in ("gw", "uw", "dw"):
        loads[name].wait()
    for copy in swaps[1:]:
        copy.wait_recv()
    for k in range(2):
        g = dot(xn[...], gw[k])
        u = dot(xn[...], uw[k])
        acts.append((g * (1.0 / (1.0 + jnp.exp(-g))) * u).astype(BF16))

    def y_copy(i, half):
        there = lax.rem(ep + i, N_EP)
        at = pl.ds(pl.multiple_of(there * CAP, CAP), CAP)
        return remote(
            ret.at[half, at, :],
            yin.at[mine, :],
            y_ssem.at[i * 2 + half],
            y_rsem.at[ep * 2 + c],
            there,
            z * 2 + half,
        )

    for half in range(2):
        cols = slice(half * HALF, (half + 1) * HALF)
        ret[half] = (dot(acts[0], dw[0, :, cols]) + dot(acts[1], dw[1, :, cols])).astype(BF16)

        def y_start(i, carry, half=half):
            y_copy(i, half).start()
            return carry

        lax.fori_loop(1, N_EP, y_start, 0)
    y_copy(0, other).start()
    yin[mine, :] = ret[c, here, :]

    def y_wait(i, carry):
        src = lax.rem(ep + i, N_EP)
        for core in range(2):
            at = pl.ds(pl.multiple_of((src * 2 + core) * CAP, CAP), CAP)
            remote(
                ret.at[core, here, :],
                yin.at[at, :],
                y_ssem.at[i * 2 + core],
                y_rsem.at[src * 2 + core],
                src,
                z * 2 + core,
            ).wait_recv()
        return carry

    theirs = pl.ds(pl.multiple_of((ep * 2 + other) * CAP, CAP), CAP)
    remote(
        ret.at[other, here, :],
        yin.at[theirs, :],
        y_ssem.at[other],
        y_rsem.at[ep * 2 + other],
        ep,
        partner,
    ).wait_recv()
    lax.fori_loop(1, N_EP, y_wait, 0)

    both = dot(comb[...], yin[...])
    moe = both[0:ROWS] + both[ROWS:]
    for zz in range(NZ):
        piece = moe[:, zz * SHARE : (zz + 1) * SHARE]
        acc[zz] = piece
        rs2_send[zz] = piece.astype(BF16)
    scatter(rs2_send, rs2_recv, rs2_ssem, rs2_rsem)
    total = after[z].astype(F32) + scatter_wait(rs2_send, rs2_recv, rs2_ssem, rs2_rsem, acc[z])
    fin[c, z] = total.astype(BF16)

    def f_copy(i):
        return remote(
            fin.at[c, z], fin.at[c, z], f_ssem.at[i], f_rsem.at[z], ep, ring(i) * 2 + c
        )

    def p_copy(zz, i):
        return remote(fin.at[c, zz], fin.at[c, zz], p_ssem.at[i], p_rsem.at[zz], ep, partner)

    for i in order:
        f_copy(i).start()
    p_copy(z, 0).start()
    for i in reversed(order):
        src = ring(i)
        remote(
            fin.at[c, src], fin.at[c, src], f_ssem.at[i], f_rsem.at[src], ep, src * 2 + c
        ).wait_recv()
        p_copy(src, i).start()

    def spread(core, zz):
        at = pl.ds(pl.multiple_of(core * HALF + zz * SHARE, SHARE), SHARE)
        mixed_out[:, at] = fin[core, zz]

    for zz in range(NZ):
        spread(c, zz)
    for i in (0,) + order[::-1]:
        src = ring(i)
        remote(
            fin.at[other, src], fin.at[other, src], p_ssem.at[i], p_rsem.at[src], ep, partner
        ).wait_recv()
        spread(other, src)

    for copy in swaps:
        copy.wait_send()

    def hv_drain(i, carry):
        hv_copy(i).wait_send()
        return carry

    lax.fori_loop(1, N_TP, hv_drain, 0)
    for i in order:
        to = ring(i)
        remote(rs_send.at[to], rs_recv.at[z], rs_ssem.at[i], rs_rsem.at[z], ep, to * 2 + c).wait_send()
        ag_copy(i, z).wait_send()
        remote(
            rs2_send.at[to], rs2_recv.at[z], rs2_ssem.at[i], rs2_rsem.at[z], ep, to * 2 + c
        ).wait_send()
        f_copy(i).wait_send()
        p_copy(ring(i), i).wait_send()
    p_copy(z, 0).wait_send()
    to_partner.wait_send()
    x_copy(0, other).wait_send()
    y_copy(0, other).wait_send()

    def xy_drain(i, carry):
        for core in range(2):
            x_copy(i, core).wait_send()
            y_copy(i, core).wait_send()
        return carry

    lax.fori_loop(1, N_EP, xy_drain, 0)


def on_device(
    residual,
    cache_latent,
    cache_rope,
    lengths,
    query_latent,
    query_rope,
    norm_gain,
    latent_weight,
    latent_gain,
    rope_weight,
    value_weight,
    out_weight,
    mixer_gain,
    group_router,
    expert_router,
    expert_ids,
    gate_weight,
    up_weight,
    down_weight,
):
    anywhere = pl.BlockSpec(memory_space=pl.ANY)
    vmem = pl.BlockSpec(memory_space=pltpu.VMEM)
    smem = pl.BlockSpec(memory_space=pltpu.SMEM)
    dma = pltpu.SemaphoreType.DMA
    in_specs = [anywhere] * 19
    in_specs[3] = smem
    return pl.pallas_call(
        kernel,
        out_shape=(
            jax.ShapeDtypeStruct((ROWS, D), BF16),
            jax.ShapeDtypeStruct((SEQS, KV), BF16),
            jax.ShapeDtypeStruct((SEQS, ROPE), BF16),
        ),
        in_specs=in_specs,
        out_specs=(vmem, vmem, vmem),
        scratch_shapes=[
            pltpu.VMEM((8, D), BF16),
            pltpu.VMEM((ROWS, SHARE), BF16),
            pltpu.VMEM((SEQS, LEN, KV), BF16),
            pltpu.VMEM((SEQS, ROPE, LEN), BF16),
            pltpu.VMEM((SEQS, H, KV), BF16),
            pltpu.VMEM((SEQS, H, ROPE), BF16),
            pltpu.VMEM((1, D), BF16),
            pltpu.VMEM((D, KV), BF16),
            pltpu.VMEM((1, KV), BF16),
            pltpu.VMEM((ROPE, D), BF16),
            pltpu.VMEM((KV, D), BF16),
            pltpu.VMEM((2, SHARE, HALF), BF16),
            pltpu.VMEM((1, D), BF16),
            pltpu.VMEM((GROUPS, D), BF16),
            pltpu.VMEM((EXPERTS, D), BF16),
            pltpu.VMEM((2, ROWS), I32),
            pltpu.VMEM((2, D, HID), BF16),
            pltpu.VMEM((2, D, HID), BF16),
            pltpu.VMEM((2, HID, D), BF16),
            pltpu.VMEM((SEQS * H, KV), BF16),
            pltpu.VMEM((NZ, 8, SHARE), BF16),
            pltpu.VMEM((N_TP, 8, SHARE), BF16),
            pltpu.VMEM((NZ, ROWS, SHARE), F32),
            pltpu.VMEM((NZ, ROWS, SHARE), BF16),
            pltpu.VMEM((NZ, ROWS, SHARE), BF16),
            pltpu.VMEM((NZ, ROWS, SHARE), BF16),
            pltpu.VMEM((NZ, ROWS, SHARE), BF16),
            pltpu.VMEM((ROWS, D), BF16),
            pltpu.VMEM((SLOTS, ROWS), BF16),
            pltpu.VMEM((SLOTS, HALF), BF16),
            pltpu.VMEM((2, N_EP * CAP, HALF), BF16),
            pltpu.VMEM((N_EP * CAP, D), BF16),
            pltpu.VMEM((2, N_EP * CAP, HALF), BF16),
            pltpu.VMEM((SLOTS, HALF), BF16),
            pltpu.VMEM((2 * ROWS, SLOTS), BF16),
            pltpu.VMEM((NZ, ROWS, SHARE), BF16),
            pltpu.VMEM((NZ, ROWS, SHARE), BF16),
            pltpu.VMEM((2, NZ, ROWS, SHARE), BF16),
            dma((32,)),
            dma((4,)),
            dma((4,)),
            dma((N_TP,)),
            dma((N_TP,)),
            dma((NZ,)),
            dma((NZ,)),
            dma((NZ,)),
            dma((NZ,)),
            dma,
            dma,
            dma((2 * N_EP,)),
            dma((2 * N_EP,)),
            dma((2 * N_EP,)),
            dma((2 * N_EP,)),
            dma((NZ,)),
            dma((NZ,)),
            dma((NZ,)),
            dma((NZ,)),
            dma((NZ,)),
            dma((NZ,)),
        ],
        compiler_params=pltpu.CompilerParams(
            collective_id=0, has_side_effects=True, vmem_limit_bytes=60 * 1024 * 1024
        ),
    )(
        residual,
        cache_latent,
        cache_rope,
        lengths,
        query_latent,
        query_rope,
        norm_gain.reshape(1, D),
        latent_weight,
        latent_gain.reshape(1, KV),
        rope_weight,
        value_weight,
        out_weight,
        mixer_gain.reshape(1, D),
        group_router.T,
        expert_router.T,
        expert_ids.T,
        gate_weight,
        up_weight,
        down_weight,
    )


def solution(mesh):
    in_specs = (
        P("ep", None),
        P(("ep", "tp"), None, None),
        P(("ep", "tp"), None, None),
        P(("ep", "tp")),
        P(("ep", "tp"), None, None),
        P(("ep", "tp"), None, None),
        P(),
        P(),
        P(),
        P(),
        P(),
        P("tp", None),
        P(),
        P(),
        P(),
        P("ep", None),
        P("ep", None, "tp"),
        P("ep", None, "tp"),
        P("ep", "tp", None),
    )
    out_specs = (P("ep", None), P(("ep", "tp"), None), P(("ep", "tp"), None))
    return jax.shard_map(
        on_device, mesh=mesh, in_specs=in_specs, out_specs=out_specs, check_vma=False
    )
```

```python
import functools
import math

import jax
import jax.numpy as jnp
from jax import lax
from jax.experimental import pallas as pl
from jax.experimental.pallas import tpu as pltpu
from jax.sharding import PartitionSpec as P

MESH = pl.DeviceIdType.MESH
F32 = jnp.float32
BF16 = jnp.bfloat16
I32 = jnp.int32

D = 2048
HALF = D // 2
H = 32
KV = 256
ROPE = 32
NOPE = 64
V = 64
GROUPS = 4
LEN = 2048
CAP = 8
N_EP = 16
N_TP = 16
NZ = 8
SEQS = 4
ROWS = 64
EXPERTS = 32
SLOTS = EXPERTS * CAP
SHARE = 128
HID = 256
OTHERS = 2 * N_EP - 1
EPS = 1e-06
ROPE_BASE = 10000.0
ORDER = (4, 3, 5, 2, 6, 1, 7)
OUT_GROUPS = ((0, 1, 7), (2, 6), (3, 5, 4))
BACK_GROUPS = ((4, 3, 5, 2), (6, 1, 7, 0))


def spans(groups):
    at, result = 0, []
    for group in groups:
        result.append((at * SHARE, len(group) * SHARE))
        at += len(group)
    return result


def dot(a, b):
    return jnp.dot(a, b, preferred_element_type=F32)


def dot_t(a, b):
    return lax.dot_general(a, b, (((1,), (1,)), ((), ())), preferred_element_type=F32)


def iota(shape, dim):
    return lax.broadcasted_iota(I32, shape, dim)


def kernel(
    residual,
    cache_latent,
    cache_rope,
    lengths_in,
    query_latent,
    query_rope,
    norm_gain,
    latent_weight,
    latent_gain,
    rope_weight,
    value_weight,
    out_weight,
    mixer_gain,
    group_router,
    expert_router,
    ids,
    gate_weight,
    up_weight,
    down_weight,
    mixed_out,
    new_latent_out,
    new_rope_out,
    lengths,
    res8,
    res_cols,
    cl,
    cr,
    ql,
    qr,
    ng,
    lw,
    lg,
    rw,
    vw,
    ow,
    mg,
    grt,
    ert,
    idv,
    gw,
    uw,
    dw,
    mixl,
    hv_send,
    hv_recv,
    acc,
    rs_send,
    rs_recv,
    after,
    after_other,
    full,
    sel,
    disp,
    xin,
    xn,
    ret,
    yin,
    comb,
    rs2_send,
    rs2_recv,
    fin,
    gain2,
    lt,
    local_sem,
    w_ssem,
    w_rsem,
    hv_ssem,
    hv_rsem,
    rs_ssem,
    rs_rsem,
    ag_ssem,
    ag_rsem,
    ot_ssem,
    ot_rsem,
    x_ssem,
    x_rsem,
    y_ssem,
    y_rsem,
    rs2_ssem,
    rs2_rsem,
    f_ssem,
    f_rsem,
    p_ssem,
    p_rsem,
):
    ep = lax.axis_index("ep")
    tp = lax.axis_index("tp")
    z = lax.div(tp, 2)
    c = lax.rem(tp, 2)
    other = 1 - c
    partner = z * 2 + other

    def remote(src, dst, ssem, rsem, to_ep, to_tp):
        return pltpu.make_async_remote_copy(
            src_ref=src,
            dst_ref=dst,
            send_sem=ssem,
            recv_sem=rsem,
            device_id=(to_ep, to_tp),
            device_id_type=MESH,
        )

    def ring(i):
        return lax.rem(z + i, NZ)

    barrier = pltpu.get_barrier_semaphore()

    def signal_tp(i, carry):
        pl.semaphore_signal(
            barrier, inc=1, device_id=(ep, lax.rem(tp + i, N_TP)), device_id_type=MESH
        )
        return carry

    def signal_ep(i, carry):
        there = lax.rem(ep + i, N_EP)
        for core in range(2):
            pl.semaphore_signal(
                barrier, inc=1, device_id=(there, z * 2 + core), device_id_type=MESH
            )
        return carry

    loads = {}

    def load(name, src, dst):
        copy = pltpu.make_async_copy(src, dst, local_sem.at[len(loads)])
        copy.start()
        loads[name] = copy

    load("len", lengths_in, lengths)
    load("res8", residual.at[pl.ds(pl.multiple_of(z * 8, 8), 8), :], res8)
    load("ng", norm_gain, ng)
    load("lg", latent_gain, lg)
    load("rw", rope_weight, rw)
    load("qr", query_rope, qr)
    load("lw", latent_weight, lw)
    load("ql", query_latent, ql)
    for s in range(SEQS):
        load(f"cr{s}", cache_rope.at[s], cr.at[s])
        load(f"cl{s}", cache_latent.at[s], cl.at[s])

    lax.fori_loop(1, N_TP, signal_tp, 0)
    lax.fori_loop(1, N_EP, signal_ep, 0)

    loads["res8"].wait()
    loads["ng"].wait()
    rows = res8[...].astype(F32)
    inv = lax.rsqrt(jnp.mean(rows * rows, axis=1, keepdims=True) + EPS)
    normed = (rows * inv * ng[...].astype(F32)[None, :]).astype(BF16)
    loads["rw"].wait()
    rope_raw = dot_t(normed, rw[...])
    loads["lw"].wait()
    latent_raw = dot(normed, lw[...])
    inv = lax.rsqrt(jnp.mean(latent_raw * latent_raw, axis=1, keepdims=True) + EPS)
    loads["lg"].wait()
    latent8 = latent_raw * inv * lg[...].astype(F32)[None, :]

    def own_rows(v):
        first = (iota(v.shape, 0) * 0 + c) == 0
        return jnp.where(first, v, pltpu.roll(v, 4, 0))

    new_latent = own_rows(latent8).astype(BF16)
    new_latent_out[...] = new_latent[0:SEQS]
    rope_own = own_rows(rope_raw)

    loads["len"].wait()
    lane = iota((8, ROPE), 1)
    row = iota((8, ROPE), 0)
    place = lax.rem(lane, ROPE // 2).astype(F32)
    freq = jnp.exp(place * (-math.log(ROPE_BASE) / (ROPE // 2)))
    pos = jnp.zeros((8, ROPE), I32)
    for s in range(SEQS):
        pos = jnp.where(row == s, lengths[s], pos)
    angle = pos.astype(F32) * freq
    cos = jnp.cos(angle)
    sin = jnp.sin(angle)
    sin = jnp.where(lane < ROPE // 2, -sin, sin)

    def swapped(u):
        return jnp.concatenate([u[:, ROPE // 2 :], u[:, : ROPE // 2]], axis=1)

    new_rope = (rope_own * cos + swapped(rope_own) * sin).astype(BF16)
    new_rope_out[...] = new_rope[0:SEQS]
    new_latent_f = new_latent.astype(F32)
    new_rope_f = new_rope.astype(F32)

    scale = (NOPE + ROPE) ** (-0.5)
    loads["qr"].wait()
    loads["ql"].wait()
    def attend(s):
        u = qr[s].astype(F32)
        turned = (u * cos[s : s + 1] + swapped(u) * sin[s : s + 1]).astype(BF16)
        q = ql[s]
        latents = cl[s]
        lt[s] = latents.T
        score = (dot(q, lt[s]) + dot(turned, cr[s])) * scale
        keep = iota((H, LEN), 1) < lengths[s]
        score = jnp.where(keep, score, -jnp.inf)
        fresh = (
            jnp.sum(q.astype(F32) * new_latent_f[s : s + 1], axis=1, keepdims=True)
            + jnp.sum(turned.astype(F32) * new_rope_f[s : s + 1], axis=1, keepdims=True)
        ) * scale
        top = jnp.maximum(jnp.max(score, axis=1, keepdims=True), fresh)
        e = jnp.exp(score - top)
        fresh_e = jnp.exp(fresh - top)
        total = jnp.sum(e, axis=1, keepdims=True) + fresh_e
        weight = (e / total).astype(BF16)
        fresh_w = (fresh_e / total).astype(BF16).astype(F32)
        mixed = dot(weight, latents) + fresh_w * new_latent_f[s : s + 1]
        mixl[s * H : (s + 1) * H, :] = mixed.astype(BF16)

    for pair in range(0, SEQS, 2):
        for s in range(pair, pair + 2):
            loads[f"cr{s}"].wait()
            loads[f"cl{s}"].wait()
        if pair + 2 == SEQS:
            load("vw", value_weight, vw)
            load("ow", out_weight.at[:, pl.ds(pl.multiple_of(c * HALF, HALF), HALF)], ow.at[c])
            share_at = pl.multiple_of(c * HALF + z * SHARE, SHARE)
            load("res_cols", residual.at[:, pl.ds(share_at, SHARE)], res_cols)
            load("ids", ids, idv)
            load("mg", mixer_gain, mg)
            load("grt", group_router, grt)
            load("ert", expert_router, ert)
        for s in range(pair, pair + 2):
            attend(s)
    pl.semaphore_wait(barrier, 45)
    swaps = [
        remote(
            out_weight.at[:, pl.ds(pl.multiple_of(other * HALF, HALF), HALF)],
            ow.at[c],
            w_ssem.at[0],
            w_rsem.at[0],
            ep,
            partner,
        ),
        remote(gate_weight.at[other], gw.at[1], w_ssem.at[1], w_rsem.at[1], ep, partner),
        remote(up_weight.at[other], uw.at[1], w_ssem.at[2], w_rsem.at[2], ep, partner),
        remote(down_weight.at[other], dw.at[1], w_ssem.at[3], w_rsem.at[3], ep, partner),
    ]
    swaps[0].start()

    loads["vw"].wait()
    wide = dot(mixl[...], vw[...])
    own = (iota((SEQS * H, D), 1) // V) == lax.rem(iota((SEQS * H, D), 0), H)
    wide = jnp.where(own, wide, 0.0).astype(BF16)
    pick = (iota((8, SEQS * H), 1) // H) == lax.rem(iota((8, SEQS * H), 0), SEQS)
    heads = dot(pick.astype(F32).astype(BF16), wide)
    low = iota((8, SHARE), 0) < SEQS
    for zz in range(NZ):
        a = heads[:, zz * 256 : zz * 256 + 128]
        b = heads[:, zz * 256 + 128 : zz * 256 + 256]
        hv_send[zz] = jnp.where(low, a, b).astype(BF16)

    def hv_copy(i):
        there = lax.rem(tp + i, N_TP)
        return remote(
            hv_send.at[lax.div(there, 2)], hv_recv.at[tp], hv_ssem, hv_rsem.at[tp], ep, there
        )

    for i in (8, 7, 9, 6, 10, 5, 11, 4, 12, 3, 13, 2, 14, 1, 15):
        hv_copy(i).start()
    hv_recv[tp] = hv_send[z]
    swaps[1].start()
    swaps[2].start()
    load("gw", gate_weight.at[c], gw.at[0])
    load("uw", up_weight.at[c], uw.at[0])
    load("dw", down_weight.at[c], dw.at[0])

    loads["ids"].wait()
    idr = idv[...]
    e_row = [idr[k : k + 1, :] for k in range(2)]
    eye = iota((ROWS, ROWS), 0) == iota((ROWS, ROWS), 1)

    def to_col(v):
        return jnp.sum(jnp.where(eye, jnp.broadcast_to(v, (ROWS, ROWS)), 0.0), axis=1, keepdims=True)

    def to_row(v):
        return jnp.sum(jnp.where(eye, jnp.broadcast_to(v, (ROWS, ROWS)), 0.0), axis=0, keepdims=True)

    e_col = [to_col(v.astype(F32)) for v in e_row]
    expert_iota = iota((ROWS, EXPERTS), 1).astype(F32)
    hits = [(jnp.broadcast_to(v, (ROWS, EXPERTS)) == expert_iota).astype(F32) for v in e_col]
    before = (iota((ROWS, ROWS), 1) < iota((ROWS, ROWS), 0)).astype(F32).astype(BF16)
    counts = dot(before, (hits[0] + hits[1]).astype(BF16))
    slot_col = [
        e_col[k] * CAP + jnp.sum(counts * hits[k], axis=1, keepdims=True) for k in range(2)
    ]
    slot_iota = iota((SLOTS, ROWS), 0).astype(F32)
    chosen = jnp.zeros((SLOTS, ROWS), F32)
    for k in range(2):
        chosen += (jnp.broadcast_to(to_row(slot_col[k]), (SLOTS, ROWS)) == slot_iota).astype(F32)
    sel[...] = chosen.astype(BF16)

    def hv_wait(i, carry):
        src = lax.rem(tp + i, N_TP)
        remote(
            hv_send.at[0], hv_recv.at[src], hv_ssem, hv_rsem.at[src], ep, src
        ).wait_recv()
        return carry

    lax.fori_loop(1, N_TP, hv_wait, 0)

    loads["ow"].wait()
    swaps[0].wait_recv()
    heads_in = hv_recv[...].astype(F32).reshape(N_TP * 8, SHARE).astype(BF16)
    part = None
    for k in range(2):
        r = iota((ROWS, N_TP * 8), 0)
        j = iota((ROWS, N_TP * 8), 1)
        rows_k = (j == 8 * (r // SEQS) + SEQS * k + lax.rem(r, SEQS)).astype(F32).astype(BF16)
        term = dot(dot(rows_k, heads_in).astype(BF16), ow[k])
        part = term if part is None else part + term
    for zz in range(NZ):
        acc[zz] = part[:, zz * SHARE : (zz + 1) * SHARE]
    for i in ORDER:
        rs_send[i] = acc[ring(i)].astype(BF16)

    def scatter_copy(send, recv, ssem, rsem, i):
        return remote(send.at[i], recv.at[z], ssem.at[i], rsem.at[z], ep, ring(i) * 2 + c)

    def scatter(send, recv, ssem, rsem, steps):
        for i in steps:
            scatter_copy(send, recv, ssem, rsem, i).start()

    def scatter_wait(send, recv, ssem, rsem, total):
        for i in reversed(ORDER):
            src = ring(i)
            remote(
                send.at[i], recv.at[src], ssem.at[i], rsem.at[src], ep, src * 2 + c
            ).wait_recv()
            total += recv[src].astype(F32)
        return total

    scatter(rs_send, rs_recv, rs_ssem, rs_rsem, ORDER)
    swaps[3].start()
    loads["res_cols"].wait()
    total = res_cols[...].astype(F32) + scatter_wait(rs_send, rs_recv, rs_ssem, rs_rsem, acc[z])
    after[z] = total.astype(BF16)

    def ag_copy(i, src):
        return remote(
            after.at[src], after.at[src], ag_ssem.at[i], ag_rsem.at[src], ep, ring(i) * 2 + c
        )

    for i in ORDER:
        ag_copy(i, z).start()

    mine = pl.ds(pl.multiple_of((ep * 2 + c) * CAP, CAP), CAP)
    here = pl.ds(pl.multiple_of(ep * CAP, CAP), CAP)
    theirs = pl.ds(pl.multiple_of((ep * 2 + other) * CAP, CAP), CAP)

    def x_copy(n, i, core):
        there = lax.rem(ep + i, N_EP)
        at = pl.ds(pl.multiple_of((there * 2 + core) * CAP, CAP), CAP)
        cols = pl.ds(*spans(OUT_GROUPS)[n])
        return remote(
            disp.at[at, cols],
            xin.at[c, here, cols],
            x_ssem.at[n],
            x_rsem.at[n, ep * 2 + c],
            there,
            z * 2 + core,
        )

    for n, group in enumerate(OUT_GROUPS):
        base = spans(OUT_GROUPS)[n][0]
        for place_at, i in enumerate(group):
            src = ring(i)
            if i:
                remote(
                    after.at[z], after.at[src], ag_ssem.at[i], ag_rsem.at[src], ep, src * 2 + c
                ).wait_recv()
            at = base + place_at * SHARE
            disp[:, at : at + SHARE] = dot(sel[...], after[src]).astype(BF16)

        def x_start(i, carry, n=n):
            for core in range(2):
                x_copy(n, i, core).start()
            return carry

        lax.fori_loop(1, N_EP, x_start, 0)
        x_copy(n, 0, other).start()
    xin[c, here, :] = disp[mine, :]
    to_partner = remote(after, after_other, ot_ssem, ot_rsem, ep, partner)
    to_partner.start()

    loads["mg"].wait()
    loads["grt"].wait()
    loads["ert"].wait()
    to_partner.wait_recv()
    for zz in range(NZ):
        at = pl.ds(pl.multiple_of(c * HALF + zz * SHARE, SHARE), SHARE)
        full[:, at] = after[zz]
        at = pl.ds(pl.multiple_of(other * HALF + zz * SHARE, SHARE), SHARE)
        full[:, at] = after_other[zz]
    gain = mg[...].astype(F32)[None, :]
    gain2[...] = gain
    rows = full[...].astype(F32)
    inv = lax.rsqrt(jnp.mean(rows * rows, axis=1, keepdims=True) + EPS)
    expert_in = (rows * inv * gain).astype(BF16)
    group_logits = dot_t(expert_in, grt[...])
    expert_logits = dot_t(expert_in, ert[...])
    group_of = jnp.floor(e_col[0] * (GROUPS / EXPERTS))
    group_hit = jnp.broadcast_to(group_of, (ROWS, GROUPS)) == iota((ROWS, GROUPS), 1).astype(F32)
    group_pick = jnp.sum(jnp.where(group_hit, group_logits, 0.0), axis=1, keepdims=True)
    share = 1.0 / jnp.sum(jnp.exp(group_logits - group_pick), axis=1, keepdims=True)
    picked = [jnp.sum(hits[k] * expert_logits, axis=1, keepdims=True) for k in range(2)]
    weights = jnp.zeros((ROWS, SLOTS), F32)
    wide_iota = iota((ROWS, SLOTS), 1).astype(F32)
    for k in range(2):
        inner = 1.0 / (1.0 + jnp.exp(picked[1 - k] - picked[k]))
        weights += jnp.where(
            jnp.broadcast_to(slot_col[k], (ROWS, SLOTS)) == wide_iota, share * inner, 0.0
        )
    high = weights.astype(BF16)
    comb[0:ROWS, :] = high
    comb[ROWS:, :] = (weights - high.astype(F32)).astype(BF16)

    def x_arrival(n, i, core):
        src = lax.rem(ep + i, N_EP)
        at = pl.ds(pl.multiple_of(src * CAP, CAP), CAP)
        cols = pl.ds(*spans(OUT_GROUPS)[n])
        return remote(
            disp.at[at, cols],
            xin.at[core, at, cols],
            x_ssem.at[n],
            x_rsem.at[n, src * 2 + core],
            src,
            z * 2 + core,
        )

    for n in range(len(OUT_GROUPS)):

        def x_wait(i, carry, n=n):
            for core in range(2):
                x_arrival(n, i, core).wait_recv()
            return carry

        x_arrival(n, 0, other).wait_recv()
        lax.fori_loop(1, N_EP, x_wait, 0)
    x0 = xin[0].astype(F32)
    x1 = xin[1].astype(F32)
    square = jnp.sum(x0 * x0, axis=1, keepdims=True) + jnp.sum(x1 * x1, axis=1, keepdims=True)
    inv = lax.rsqrt(square * (1.0 / D) + EPS)
    for core in range(2):
        for place_at, i in enumerate(sum(OUT_GROUPS, ())):
            at = pl.ds(pl.multiple_of(core * HALF + ring(i) * SHARE, SHARE), SHARE)
            piece = xin[core, :, place_at * SHARE : (place_at + 1) * SHARE].astype(F32)
            xn[:, at] = (piece * inv * gain2[:, at]).astype(BF16)
    acts = []
    for name in ("gw", "uw", "dw"):
        loads[name].wait()
    for copy in swaps[1:]:
        copy.wait_recv()
    for k in range(2):
        g = dot(xn[...], gw[k])
        u = dot(xn[...], uw[k])
        acts.append((g * (1.0 / (1.0 + jnp.exp(-g))) * u).astype(BF16))

    def y_copy(n, i, half):
        there = lax.rem(ep + i, N_EP)
        at = pl.ds(pl.multiple_of(there * CAP, CAP), CAP)
        cols = pl.ds(*spans(BACK_GROUPS)[n])
        return remote(
            ret.at[half, at, cols],
            yin.at[mine, cols],
            y_ssem.at[n],
            y_rsem.at[n, ep * 2 + c],
            there,
            z * 2 + half,
        )

    for n, group in enumerate(BACK_GROUPS):
        base = spans(BACK_GROUPS)[n][0]
        for half in range(2):
            for place_at, i in enumerate(group):
                at = pl.ds(pl.multiple_of(half * HALF + ring(i) * SHARE, SHARE), SHARE)
                to = base + place_at * SHARE
                ret[half, :, to : to + SHARE] = (
                    dot(acts[0], dw[0, :, at]) + dot(acts[1], dw[1, :, at])
                ).astype(BF16)

        def y_start(i, carry, n=n):
            for half in range(2):
                y_copy(n, i, half).start()
            return carry

        lax.fori_loop(1, N_EP, y_start, 0)
        y_copy(n, 0, other).start()
    yin[mine, :] = ret[c, here, :]

    def y_arrival(n, i, core):
        src = lax.rem(ep + i, N_EP)
        at = pl.ds(pl.multiple_of((src * 2 + core) * CAP, CAP), CAP)
        cols = pl.ds(*spans(BACK_GROUPS)[n])
        return remote(
            ret.at[core, here, cols],
            yin.at[at, cols],
            y_ssem.at[n],
            y_rsem.at[n, src * 2 + core],
            src,
            z * 2 + core,
        )

    for n, group in enumerate(BACK_GROUPS):

        def y_wait(i, carry, n=n):
            for core in range(2):
                y_arrival(n, i, core).wait_recv()
            return carry

        y_arrival(n, 0, other).wait_recv()
        lax.fori_loop(1, N_EP, y_wait, 0)
        base, width = spans(BACK_GROUPS)[n]
        both = dot(comb[...], yin[:, base : base + width])
        moe = both[0:ROWS] + both[ROWS:]
        for place_at, i in enumerate(group):
            piece = moe[:, place_at * SHARE : (place_at + 1) * SHARE]
            if i:
                rs2_send[i] = piece.astype(BF16)
                scatter(rs2_send, rs2_recv, rs2_ssem, rs2_rsem, (i,))
            else:
                acc[0] = piece
    total = after[z].astype(F32) + scatter_wait(rs2_send, rs2_recv, rs2_ssem, rs2_rsem, acc[0])
    fin[c, z] = total.astype(BF16)

    def f_copy(i):
        return remote(
            fin.at[c, z], fin.at[c, z], f_ssem.at[i], f_rsem.at[z], ep, ring(i) * 2 + c
        )

    def p_copy(zz, i):
        return remote(fin.at[c, zz], fin.at[c, zz], p_ssem.at[i], p_rsem.at[zz], ep, partner)

    for i in ORDER:
        f_copy(i).start()
    p_copy(z, 0).start()
    for i in reversed(ORDER):
        src = ring(i)
        remote(
            fin.at[c, src], fin.at[c, src], f_ssem.at[i], f_rsem.at[src], ep, src * 2 + c
        ).wait_recv()
        p_copy(src, i).start()

    def spread(core, zz):
        at = pl.ds(pl.multiple_of(core * HALF + zz * SHARE, SHARE), SHARE)
        mixed_out[:, at] = fin[core, zz]

    for zz in range(NZ):
        spread(c, zz)
    for i in (0,) + ORDER[::-1]:
        src = ring(i)
        remote(
            fin.at[other, src], fin.at[other, src], p_ssem.at[i], p_rsem.at[src], ep, partner
        ).wait_recv()
        spread(other, src)

    for copy in swaps:
        copy.wait_send()
    remote(
        hv_recv.at[0 : N_TP - 1], hv_recv.at[0 : N_TP - 1], hv_ssem, hv_rsem.at[0], ep, partner
    ).wait_send()
    for i in ORDER:
        scatter_copy(rs_send, rs_recv, rs_ssem, rs_rsem, i).wait_send()
        ag_copy(i, z).wait_send()
        scatter_copy(rs2_send, rs2_recv, rs2_ssem, rs2_rsem, i).wait_send()
        f_copy(i).wait_send()
        p_copy(ring(i), i).wait_send()
    p_copy(z, 0).wait_send()
    to_partner.wait_send()
    sent = pl.ds(0, OTHERS * CAP)
    for n, span in enumerate(spans(OUT_GROUPS)):
        part_of = disp.at[sent, pl.ds(*span)]
        remote(part_of, part_of, x_ssem.at[n], x_rsem.at[n, 0], ep, partner).wait_send()
    for n, span in enumerate(spans(BACK_GROUPS)):
        part_of = yin.at[sent, pl.ds(*span)]
        remote(part_of, part_of, y_ssem.at[n], y_rsem.at[n, 0], ep, partner).wait_send()


def write_out(a, b, c, a_out, b_out, c_out, sem):
    copies = [
        pltpu.make_async_copy(src, dst, sem.at[i])
        for i, (src, dst) in enumerate(((a, a_out), (b, b_out), (c, c_out)))
    ]
    for copy in copies:
        copy.start()
    for copy in copies:
        copy.wait()


def on_device(
    residual,
    cache_latent,
    cache_rope,
    lengths,
    query_latent,
    query_rope,
    norm_gain,
    latent_weight,
    latent_gain,
    rope_weight,
    value_weight,
    out_weight,
    mixer_gain,
    group_router,
    expert_router,
    expert_ids,
    gate_weight,
    up_weight,
    down_weight,
):
    anywhere = pl.BlockSpec(memory_space=pl.ANY)
    vmem = pl.BlockSpec(memory_space=pltpu.VMEM)
    dma = pltpu.SemaphoreType.DMA
    in_specs = [anywhere] * 19
    results = pl.pallas_call(
        kernel,
        out_shape=(
            pltpu.VMEM((ROWS, D), BF16),
            pltpu.VMEM((SEQS, KV), BF16),
            pltpu.VMEM((SEQS, ROPE), BF16),
        ),
        in_specs=in_specs,
        out_specs=(vmem, vmem, vmem),
        scratch_shapes=[
            pltpu.SMEM((SEQS,), I32),
            pltpu.VMEM((8, D), BF16),
            pltpu.VMEM((ROWS, SHARE), BF16),
            pltpu.VMEM((SEQS, LEN, KV), BF16),
            pltpu.VMEM((SEQS, ROPE, LEN), BF16),
            pltpu.VMEM((SEQS, H, KV), BF16),
            pltpu.VMEM((SEQS, H, ROPE), BF16),
            pltpu.VMEM((D,), BF16),
            pltpu.VMEM((D, KV), BF16),
            pltpu.VMEM((KV,), BF16),
            pltpu.VMEM((ROPE, D), BF16),
            pltpu.VMEM((KV, D), BF16),
            pltpu.VMEM((2, SHARE, HALF), BF16),
            pltpu.VMEM((D,), BF16),
            pltpu.VMEM((GROUPS, D), BF16),
            pltpu.VMEM((EXPERTS, D), BF16),
            pltpu.VMEM((2, ROWS), I32),
            pltpu.VMEM((2, D, HID), BF16),
            pltpu.VMEM((2, D, HID), BF16),
            pltpu.VMEM((2, HID, D), BF16),
            pltpu.VMEM((SEQS * H, KV), BF16),
            pltpu.VMEM((NZ, 8, SHARE), BF16),
            pltpu.VMEM((N_TP, 8, SHARE), BF16),
            pltpu.VMEM((NZ, ROWS, SHARE), F32),
            pltpu.VMEM((NZ, ROWS, SHARE), BF16),
            pltpu.VMEM((NZ, ROWS, SHARE), BF16),
            pltpu.VMEM((NZ, ROWS, SHARE), BF16),
            pltpu.VMEM((NZ, ROWS, SHARE), BF16),
            pltpu.VMEM((ROWS, D), BF16),
            pltpu.VMEM((SLOTS, ROWS), BF16),
            pltpu.VMEM((SLOTS, HALF), BF16),
            pltpu.VMEM((2, N_EP * CAP, HALF), BF16),
            pltpu.VMEM((N_EP * CAP, D), BF16),
            pltpu.VMEM((2, N_EP * CAP, HALF), BF16),
            pltpu.VMEM((SLOTS, HALF), BF16),
            pltpu.VMEM((2 * ROWS, SLOTS), BF16),
            pltpu.VMEM((NZ, ROWS, SHARE), BF16),
            pltpu.VMEM((NZ, ROWS, SHARE), BF16),
            pltpu.VMEM((2, NZ, ROWS, SHARE), BF16),
            pltpu.VMEM((1, D), F32),
            pltpu.VMEM((SEQS, KV, LEN), BF16),
            dma((32,)),
            dma((4,)),
            dma((4,)),
            dma,
            dma((N_TP,)),
            dma((NZ,)),
            dma((NZ,)),
            dma((NZ,)),
            dma((NZ,)),
            dma,
            dma,
            dma((len(OUT_GROUPS),)),
            dma((len(OUT_GROUPS), 2 * N_EP)),
            dma((len(BACK_GROUPS),)),
            dma((len(BACK_GROUPS), 2 * N_EP)),
            dma((NZ,)),
            dma((NZ,)),
            dma((NZ,)),
            dma((NZ,)),
            dma((NZ,)),
            dma((NZ,)),
        ],
        compiler_params=pltpu.CompilerParams(
            collective_id=0, has_side_effects=True, vmem_limit_bytes=60 * 1024 * 1024
        ),
    )(
        residual,
        cache_latent,
        cache_rope,
        lengths,
        query_latent,
        query_rope,
        norm_gain,
        latent_weight,
        latent_gain,
        rope_weight,
        value_weight,
        out_weight,
        mixer_gain,
        group_router.T,
        expert_router.T,
        expert_ids.T,
        gate_weight,
        up_weight,
        down_weight,
    )
    return pl.pallas_call(
        write_out,
        out_shape=(
            jax.ShapeDtypeStruct((ROWS, D), BF16),
            jax.ShapeDtypeStruct((SEQS, KV), BF16),
            jax.ShapeDtypeStruct((SEQS, ROPE), BF16),
        ),
        in_specs=[vmem] * 3,
        out_specs=(anywhere,) * 3,
        scratch_shapes=[dma((3,))],
        compiler_params=pltpu.CompilerParams(vmem_limit_bytes=1024 * 1024),
    )(*results)


def solution(mesh):
    in_specs = (
        P("ep", None),
        P(("ep", "tp"), None, None),
        P(("ep", "tp"), None, None),
        P(("ep", "tp")),
        P(("ep", "tp"), None, None),
        P(("ep", "tp"), None, None),
        P(),
        P(),
        P(),
        P(),
        P(),
        P("tp", None),
        P(),
        P(),
        P(),
        P("ep", None),
        P("ep", None, "tp"),
        P("ep", None, "tp"),
        P("ep", "tp", None),
    )
    out_specs = (P("ep", None), P(("ep", "tp"), None), P(("ep", "tp"), None))
    return jax.shard_map(
        on_device, mesh=mesh, in_specs=in_specs, out_specs=out_specs, check_vma=False
    )
```

```python
import functools
import math

import jax
import jax.numpy as jnp
from jax import lax
from jax.experimental import pallas as pl
from jax.experimental.pallas import tpu as pltpu
from jax.sharding import PartitionSpec as P

MESH = pl.DeviceIdType.MESH
F32 = jnp.float32
BF16 = jnp.bfloat16
I32 = jnp.int32

D = 2048
HALF = D // 2
H = 32
KV = 256
ROPE = 32
NOPE = 64
V = 64
GROUPS = 4
LEN = 2048
CAP = 8
N_EP = 16
N_TP = 16
NZ = 8
SEQS = 4
ROWS = 64
EXPERTS = 32
SLOTS = EXPERTS * CAP
SHARE = 128
HID = 256
OTHERS = 2 * N_EP - 1
EPS = 1e-06
ROPE_BASE = 10000.0
ORDER = (4, 3, 5, 2, 6, 1, 7)
OUT_GROUPS = ((0,), (1, 7), (2, 6), (3, 5, 4))
BACK_GROUPS = ((4, 3, 5), (2, 6), (1, 7, 0))

FAR_FIRST = tuple(
    sorted(
        ((a, b) for a in range(4) for b in range(4) if a or b),
        key=lambda step: -sum(min(v, 4 - v) for v in step),
    )
)


def spans(groups):
    at, result = 0, []
    for group in groups:
        result.append((at * SHARE, len(group) * SHARE))
        at += len(group)
    return result


def dot(a, b):
    return jnp.dot(a, b, preferred_element_type=F32)


def dot_t(a, b):
    return lax.dot_general(a, b, (((1,), (1,)), ((), ())), preferred_element_type=F32)


def iota(shape, dim):
    return lax.broadcasted_iota(I32, shape, dim)


def kernel(
    residual,
    cache_latent,
    cache_rope,
    lengths_in,
    query_latent,
    query_rope,
    norm_gain,
    latent_weight,
    latent_gain,
    rope_weight,
    value_weight,
    out_weight,
    mixer_gain,
    group_router,
    expert_router,
    ids,
    gate_weight,
    up_weight,
    down_weight,
    mixed_out,
    new_latent_out,
    new_rope_out,
    lengths,
    res8,
    res_cols,
    cl,
    cr,
    ql,
    qr,
    ng,
    lw,
    lg,
    rw,
    vw,
    ow,
    mg,
    grt,
    ert,
    idv,
    gw,
    uw,
    dw,
    mixl,
    hv_send,
    hv_recv,
    acc,
    rs_send,
    rs_recv,
    after,
    after_other,
    full,
    sel,
    disp,
    xin,
    ret,
    yin,
    comb,
    rs2_send,
    rs2_recv,
    fin,
    gain2,
    lt,
    early,
    local_sem,
    w_ssem,
    w_rsem,
    hv_ssem,
    hv_rsem,
    rs_ssem,
    rs_rsem,
    ag_ssem,
    ag_rsem,
    ot_ssem,
    ot_rsem,
    x_ssem,
    x_rsem,
    y_ssem,
    y_rsem,
    rs2_ssem,
    rs2_rsem,
    f_ssem,
    f_rsem,
    p_ssem,
    p_rsem,
):
    ep = lax.axis_index("ep")
    tp = lax.axis_index("tp")
    z = lax.div(tp, 2)
    c = lax.rem(tp, 2)
    other = 1 - c
    partner = z * 2 + other

    def remote(src, dst, ssem, rsem, to_ep, to_tp):
        return pltpu.make_async_remote_copy(
            src_ref=src,
            dst_ref=dst,
            send_sem=ssem,
            recv_sem=rsem,
            device_id=(to_ep, to_tp),
            device_id_type=MESH,
        )

    def ring(i):
        return lax.rem(z + i, NZ)

    barrier = pltpu.get_barrier_semaphore()

    def signal_tp(i, carry):
        pl.semaphore_signal(
            barrier, inc=1, device_id=(ep, lax.rem(tp + i, N_TP)), device_id_type=MESH
        )
        return carry

    def signal_ep(i, carry):
        there = lax.rem(ep + i, N_EP)
        for core in range(2):
            pl.semaphore_signal(
                barrier, inc=1, device_id=(there, z * 2 + core), device_id_type=MESH
            )
        return carry

    loads = {}

    def load(name, src, dst):
        copy = pltpu.make_async_copy(src, dst, local_sem.at[len(loads)])
        copy.start()
        loads[name] = copy

    load("ql", query_latent, ql)
    load("cl0", cache_latent.at[0:2], cl.at[0:2])
    load("len", lengths_in, lengths)
    load("res8", residual.at[pl.ds(pl.multiple_of(z * 8, 8), 8), :], res8)
    load("ng", norm_gain, ng)
    load("lg", latent_gain, lg)
    load("rw", rope_weight, rw)
    load("qr", query_rope, qr)
    load("lw", latent_weight, lw)
    load("cr", cache_rope, cr)
    load("cl2", cache_latent.at[2:4], cl.at[2:4])

    lax.fori_loop(1, N_TP, signal_tp, 0)
    lax.fori_loop(1, N_EP, signal_ep, 0)

    loads["ql"].wait()
    loads["cl0"].wait()
    for s in range(2):
        lt[s] = cl[s].T
        early[s] = dot(ql[s], lt[s])

    for name in ("len", "res8", "ng", "lg", "rw", "qr", "lw", "cr", "cl2"):
        loads[name].wait()
    rows = res8[...].astype(F32)
    inv = lax.rsqrt(jnp.mean(rows * rows, axis=1, keepdims=True) + EPS)
    normed = (rows * inv * ng[...].astype(F32)[None, :]).astype(BF16)
    rope_raw = dot_t(normed, rw[...])
    latent_raw = dot(normed, lw[...])
    inv = lax.rsqrt(jnp.mean(latent_raw * latent_raw, axis=1, keepdims=True) + EPS)
    latent8 = latent_raw * inv * lg[...].astype(F32)[None, :]

    def own_rows(v):
        first = (iota(v.shape, 0) * 0 + c) == 0
        return jnp.where(first, v, pltpu.roll(v, 4, 0))

    new_latent = own_rows(latent8).astype(BF16)
    new_latent_out[...] = new_latent[0:SEQS]
    rope_own = own_rows(rope_raw)

    lane = iota((8, ROPE), 1)
    row = iota((8, ROPE), 0)
    place = lax.rem(lane, ROPE // 2).astype(F32)
    freq = jnp.exp(place * (-math.log(ROPE_BASE) / (ROPE // 2)))
    pos = jnp.zeros((8, ROPE), I32)
    for s in range(SEQS):
        pos = jnp.where(row == s, lengths[s], pos)
    angle = pos.astype(F32) * freq
    cos = jnp.cos(angle)
    sin = jnp.sin(angle)
    sin = jnp.where(lane < ROPE // 2, -sin, sin)

    def swapped(u):
        return jnp.concatenate([u[:, ROPE // 2 :], u[:, : ROPE // 2]], axis=1)

    new_rope = (rope_own * cos + swapped(rope_own) * sin).astype(BF16)
    new_rope_out[...] = new_rope[0:SEQS]
    new_latent_f = new_latent.astype(F32)
    new_rope_f = new_rope.astype(F32)

    scale = (NOPE + ROPE) ** (-0.5)
    def attend(s):
        u = qr[s].astype(F32)
        turned = (u * cos[s : s + 1] + swapped(u) * sin[s : s + 1]).astype(BF16)
        q = ql[s]
        latents = cl[s]
        if s < 2:
            score = early[s]
        else:
            lt[s] = latents.T
            score = dot(q, lt[s])
        score = (score + dot(turned, cr[s])) * scale
        keep = iota((H, LEN), 1) < lengths[s]
        score = jnp.where(keep, score, -jnp.inf)
        fresh = (
            jnp.sum(q.astype(F32) * new_latent_f[s : s + 1], axis=1, keepdims=True)
            + jnp.sum(turned.astype(F32) * new_rope_f[s : s + 1], axis=1, keepdims=True)
        ) * scale
        top = jnp.maximum(jnp.max(score, axis=1, keepdims=True), fresh)
        e = jnp.exp(score - top)
        fresh_e = jnp.exp(fresh - top)
        total = jnp.sum(e, axis=1, keepdims=True) + fresh_e
        weight = (e / total).astype(BF16)
        fresh_w = (fresh_e / total).astype(BF16).astype(F32)
        mixed = dot(weight, latents) + fresh_w * new_latent_f[s : s + 1]
        mixl[s * H : (s + 1) * H, :] = mixed.astype(BF16)

    load("vw", value_weight, vw)
    load("ow", out_weight.at[:, pl.ds(pl.multiple_of(c * HALF, HALF), HALF)], ow.at[c])
    share_at = pl.multiple_of(c * HALF + z * SHARE, SHARE)
    load("res_cols", residual.at[:, pl.ds(share_at, SHARE)], res_cols)
    load("ids", ids, idv)
    load("mg", mixer_gain, mg)
    load("grt", group_router, grt)
    load("ert", expert_router, ert)
    for s in range(SEQS):
        attend(s)
    pl.semaphore_wait(barrier, 45)
    swaps = [
        remote(
            out_weight.at[:, pl.ds(pl.multiple_of(other * HALF, HALF), HALF)],
            ow.at[c],
            w_ssem.at[0],
            w_rsem.at[0],
            ep,
            partner,
        ),
        remote(gate_weight.at[other], gw.at[1], w_ssem.at[1], w_rsem.at[1], ep, partner),
        remote(up_weight.at[other], uw.at[1], w_ssem.at[2], w_rsem.at[2], ep, partner),
        remote(down_weight.at[other], dw.at[1], w_ssem.at[3], w_rsem.at[3], ep, partner),
    ]
    swaps[0].start()

    loads["vw"].wait()
    wide = dot(mixl[...], vw[...])
    own = (iota((SEQS * H, D), 1) // V) == lax.rem(iota((SEQS * H, D), 0), H)
    wide = jnp.where(own, wide, 0.0).astype(BF16)
    pick = (iota((8, SEQS * H), 1) // H) == lax.rem(iota((8, SEQS * H), 0), SEQS)
    heads = dot(pick.astype(F32).astype(BF16), wide)
    low = iota((8, SHARE), 0) < SEQS
    for zz in range(NZ):
        a = heads[:, zz * 256 : zz * 256 + 128]
        b = heads[:, zz * 256 + 128 : zz * 256 + 256]
        hv_send[zz] = jnp.where(low, a, b).astype(BF16)

    def hv_copy(i):
        there = lax.rem(tp + i, N_TP)
        return remote(
            hv_send.at[lax.div(there, 2)], hv_recv.at[tp], hv_ssem, hv_rsem, ep, there
        )

    for i in (8, 7, 9, 6, 10, 5, 11, 4, 12, 3, 13, 2, 14, 1, 15):
        hv_copy(i).start()
    hv_recv[tp] = hv_send[z]
    swaps[1].start()
    swaps[2].start()
    load("gw", gate_weight.at[c], gw.at[0])
    load("uw", up_weight.at[c], uw.at[0])
    load("dw", down_weight.at[c], dw.at[0])

    loads["ids"].wait()
    idr = idv[...]
    e_row = [idr[k : k + 1, :] for k in range(2)]
    eye = iota((ROWS, ROWS), 0) == iota((ROWS, ROWS), 1)

    def to_col(v):
        return jnp.sum(jnp.where(eye, jnp.broadcast_to(v, (ROWS, ROWS)), 0.0), axis=1, keepdims=True)

    def to_row(v):
        return jnp.sum(jnp.where(eye, jnp.broadcast_to(v, (ROWS, ROWS)), 0.0), axis=0, keepdims=True)

    e_col = [to_col(v.astype(F32)) for v in e_row]
    expert_iota = iota((ROWS, EXPERTS), 1).astype(F32)
    hits = [(jnp.broadcast_to(v, (ROWS, EXPERTS)) == expert_iota).astype(F32) for v in e_col]
    before = (iota((ROWS, ROWS), 1) < iota((ROWS, ROWS), 0)).astype(F32).astype(BF16)
    counts = dot(before, (hits[0] + hits[1]).astype(BF16))
    slot_col = [
        e_col[k] * CAP + jnp.sum(counts * hits[k], axis=1, keepdims=True) for k in range(2)
    ]
    slot_iota = iota((SLOTS, ROWS), 0).astype(F32)
    chosen = jnp.zeros((SLOTS, ROWS), F32)
    for k in range(2):
        chosen += (jnp.broadcast_to(to_row(slot_col[k]), (SLOTS, ROWS)) == slot_iota).astype(F32)
    sel[...] = chosen.astype(BF16)

    all_heads = hv_recv.at[0 : N_TP - 1]
    remote(all_heads, all_heads, hv_ssem, hv_rsem, ep, partner).wait_recv()

    loads["ow"].wait()
    swaps[0].wait_recv()
    heads_in = hv_recv[...].astype(F32).reshape(N_TP * 8, SHARE).astype(BF16)
    part = None
    for k in range(2):
        r = iota((ROWS, N_TP * 8), 0)
        j = iota((ROWS, N_TP * 8), 1)
        rows_k = (j == 8 * (r // SEQS) + SEQS * k + lax.rem(r, SEQS)).astype(F32).astype(BF16)
        term = dot(dot(rows_k, heads_in).astype(BF16), ow[k])
        part = term if part is None else part + term
    for zz in range(NZ):
        acc[zz] = part[:, zz * SHARE : (zz + 1) * SHARE]
    for i in ORDER:
        rs_send[i] = acc[ring(i)].astype(BF16)

    def scatter_copy(send, recv, ssem, rsem, i):
        return remote(send.at[i], recv.at[z], ssem, rsem, ep, ring(i) * 2 + c)

    def scatter(send, recv, ssem, rsem, steps):
        for i in steps:
            scatter_copy(send, recv, ssem, rsem, i).start()

    def scatter_all(recv, ssem, rsem):
        seven = recv.at[0 : NZ - 1]
        return remote(seven, seven, ssem, rsem, ep, partner)

    def scatter_wait(recv, ssem, rsem, total):
        scatter_all(recv, ssem, rsem).wait_recv()
        for i in ORDER:
            total += recv[ring(i)].astype(F32)
        return total

    scatter(rs_send, rs_recv, rs_ssem, rs_rsem, ORDER)
    swaps[3].start()
    loads["res_cols"].wait()
    total = res_cols[...].astype(F32) + scatter_wait(rs_recv, rs_ssem, rs_rsem, acc[z])
    after[z] = total.astype(BF16)

    def group_of(i):
        return [i in group for group in OUT_GROUPS].index(True)

    def ag_copy(i):
        return remote(
            after.at[z], after.at[z], ag_ssem, ag_rsem.at[group_of(NZ - i)], ep, ring(i) * 2 + c
        )

    for i in ORDER:
        ag_copy(i).start()

    mine = pl.ds(pl.multiple_of((ep * 2 + c) * CAP, CAP), CAP)
    here = pl.ds(pl.multiple_of(ep * CAP, CAP), CAP)
    theirs = pl.ds(pl.multiple_of((ep * 2 + other) * CAP, CAP), CAP)

    def away(step):
        down, right = step
        return lax.rem(lax.div(ep, 4) + down, 4) * 4 + lax.rem(ep + right, 4)

    def x_copy(n, step, core):
        there = away(step)
        at = pl.ds(pl.multiple_of((there * 2 + core) * CAP, CAP), CAP)
        cols = pl.ds(*spans(OUT_GROUPS)[n])
        return remote(
            disp.at[at, cols],
            xin.at[c, here, cols],
            x_ssem.at[n],
            x_rsem.at[n],
            there,
            z * 2 + core,
        )

    for n, group in enumerate(OUT_GROUPS):
        base = spans(OUT_GROUPS)[n][0]
        come = after.at[0 : max(1, len(group) - (0 in group))]
        if group != (0,):
            remote(come, come, ag_ssem, ag_rsem.at[n], ep, partner).wait_recv()
        for place_at, i in enumerate(group):
            at = base + place_at * SHARE
            disp[:, at : at + SHARE] = dot(sel[...], after[ring(i)]).astype(BF16)
        for step in FAR_FIRST:
            for core in range(2):
                x_copy(n, step, core).start()
        x_copy(n, (0, 0), other).start()
    xin[c, here, :] = disp[mine, :]
    to_partner = remote(after, after_other, ot_ssem, ot_rsem, ep, partner)
    to_partner.start()

    loads["mg"].wait()
    loads["grt"].wait()
    loads["ert"].wait()
    to_partner.wait_recv()
    for zz in range(NZ):
        at = pl.ds(pl.multiple_of(c * HALF + zz * SHARE, SHARE), SHARE)
        full[:, at] = after[zz]
        at = pl.ds(pl.multiple_of(other * HALF + zz * SHARE, SHARE), SHARE)
        full[:, at] = after_other[zz]
    gain = mg[...].astype(F32)[None, :]
    gain2[...] = gain
    rows = full[...].astype(F32)
    inv = lax.rsqrt(jnp.mean(rows * rows, axis=1, keepdims=True) + EPS)
    expert_in = (rows * inv * gain).astype(BF16)
    group_logits = dot_t(expert_in, grt[...])
    expert_logits = dot_t(expert_in, ert[...])
    group_of = jnp.floor(e_col[0] * (GROUPS / EXPERTS))
    group_hit = jnp.broadcast_to(group_of, (ROWS, GROUPS)) == iota((ROWS, GROUPS), 1).astype(F32)
    group_pick = jnp.sum(jnp.where(group_hit, group_logits, 0.0), axis=1, keepdims=True)
    share = 1.0 / jnp.sum(jnp.exp(group_logits - group_pick), axis=1, keepdims=True)
    picked = [jnp.sum(hits[k] * expert_logits, axis=1, keepdims=True) for k in range(2)]
    weights = jnp.zeros((ROWS, SLOTS), F32)
    wide_iota = iota((ROWS, SLOTS), 1).astype(F32)
    for k in range(2):
        inner = 1.0 / (1.0 + jnp.exp(picked[1 - k] - picked[k]))
        weights += jnp.where(
            jnp.broadcast_to(slot_col[k], (ROWS, SLOTS)) == wide_iota, share * inner, 0.0
        )
    high = weights.astype(BF16)
    comb[0:ROWS, :] = high
    comb[ROWS:, :] = (weights - high.astype(F32)).astype(BF16)

    sent = pl.ds(0, OTHERS * CAP)

    def x_all(n):
        part_of = disp.at[sent, pl.ds(*spans(OUT_GROUPS)[n])]
        return remote(part_of, part_of, x_ssem.at[n], x_rsem.at[n], ep, partner)

    def y_all(n):
        part_of = yin.at[sent, pl.ds(*spans(BACK_GROUPS)[n])]
        return remote(part_of, part_of, y_ssem.at[n], y_rsem.at[n], ep, partner)

    for name in ("gw", "uw"):
        loads[name].wait()
    swaps[1].wait_recv()
    swaps[2].wait_recv()
    products = [0.0, 0.0, 0.0, 0.0]
    square = 0.0
    for n, group in enumerate(OUT_GROUPS):
        x_all(n).wait_recv()
        base = spans(OUT_GROUPS)[n][0]
        for core in range(2):
            for place_at, i in enumerate(group):
                at = pl.ds(pl.multiple_of(core * HALF + ring(i) * SHARE, SHARE), SHARE)
                to = base + place_at * SHARE
                piece = xin[core, :, to : to + SHARE].astype(F32)
                square += piece * piece
                scaled = (piece * gain2[:, at]).astype(BF16)
                for k in range(2):
                    products[k] += dot(scaled, gw[k, at, :])
                    products[2 + k] += dot(scaled, uw[k, at, :])
    inv = lax.rsqrt(jnp.sum(square, axis=1, keepdims=True) * (1.0 / D) + EPS)
    acts = []
    for k in range(2):
        g = products[k] * inv
        u = products[2 + k] * inv
        acts.append((g * (1.0 / (1.0 + jnp.exp(-g))) * u).astype(BF16))
    loads["dw"].wait()
    swaps[3].wait_recv()

    def y_copy(n, step, half):
        there = away(step)
        at = pl.ds(pl.multiple_of(there * CAP, CAP), CAP)
        cols = pl.ds(*spans(BACK_GROUPS)[n])
        return remote(
            ret.at[half, at, cols],
            yin.at[mine, cols],
            y_ssem.at[n],
            y_rsem.at[n],
            there,
            z * 2 + half,
        )

    for n, group in enumerate(BACK_GROUPS):
        base = spans(BACK_GROUPS)[n][0]
        for half in range(2):
            for place_at, i in enumerate(group):
                at = pl.ds(pl.multiple_of(half * HALF + ring(i) * SHARE, SHARE), SHARE)
                to = base + place_at * SHARE
                ret[half, :, to : to + SHARE] = (
                    dot(acts[0], dw[0, :, at]) + dot(acts[1], dw[1, :, at])
                ).astype(BF16)

        for step in FAR_FIRST:
            for half in range(2):
                y_copy(n, step, half).start()
        y_copy(n, (0, 0), other).start()
    yin[mine, :] = ret[c, here, :]

    for n, group in enumerate(BACK_GROUPS):
        y_all(n).wait_recv()
        base, width = spans(BACK_GROUPS)[n]
        both = dot(comb[...], yin[:, base : base + width])
        moe = both[0:ROWS] + both[ROWS:]
        for place_at, i in enumerate(group):
            piece = moe[:, place_at * SHARE : (place_at + 1) * SHARE]
            if i:
                rs2_send[i] = piece.astype(BF16)
                scatter(rs2_send, rs2_recv, rs2_ssem, rs2_rsem, (i,))
            else:
                acc[0] = piece
    total = after[z].astype(F32) + scatter_wait(rs2_recv, rs2_ssem, rs2_rsem, acc[0])
    fin[c, z] = total.astype(BF16)

    def f_copy(i):
        return remote(
            fin.at[c, z], fin.at[c, z], f_ssem, f_rsem.at[z], ep, ring(i) * 2 + c
        )

    def p_copy(zz):
        return remote(fin.at[c, zz], fin.at[c, zz], p_ssem, p_rsem, ep, partner)

    for i in ORDER:
        f_copy(i).start()
    p_copy(z).start()
    for i in reversed(ORDER):
        src = ring(i)
        remote(
            fin.at[c, src], fin.at[c, src], f_ssem, f_rsem.at[src], ep, src * 2 + c
        ).wait_recv()
        p_copy(src).start()

    def spread(core, zz):
        at = pl.ds(pl.multiple_of(core * HALF + zz * SHARE, SHARE), SHARE)
        mixed_out[:, at] = fin[core, zz]

    for zz in range(NZ):
        spread(c, zz)
    remote(fin.at[other], fin.at[other], p_ssem, p_rsem, ep, partner).wait_recv()
    for zz in range(NZ):
        spread(other, zz)

    for copy in swaps:
        copy.wait_send()
    remote(all_heads, all_heads, hv_ssem, hv_rsem, ep, partner).wait_send()
    scatter_all(rs_recv, rs_ssem, rs_rsem).wait_send()
    scatter_all(rs2_recv, rs2_ssem, rs2_rsem).wait_send()
    scatter_all(after, ag_ssem, rs_rsem).wait_send()
    scatter_all(rs_recv, f_ssem, rs_rsem).wait_send()
    remote(fin.at[other], fin.at[other], p_ssem, p_rsem, ep, partner).wait_send()
    to_partner.wait_send()
    for n in range(len(OUT_GROUPS)):
        x_all(n).wait_send()
    for n in range(len(BACK_GROUPS)):
        y_all(n).wait_send()


def write_out(a, b, c, a_out, b_out, c_out, sem):
    copies = [
        pltpu.make_async_copy(src, dst, sem.at[i])
        for i, (src, dst) in enumerate(((a, a_out), (b, b_out), (c, c_out)))
    ]
    for copy in copies:
        copy.start()
    for copy in copies:
        copy.wait()


def on_device(
    residual,
    cache_latent,
    cache_rope,
    lengths,
    query_latent,
    query_rope,
    norm_gain,
    latent_weight,
    latent_gain,
    rope_weight,
    value_weight,
    out_weight,
    mixer_gain,
    group_router,
    expert_router,
    expert_ids,
    gate_weight,
    up_weight,
    down_weight,
):
    anywhere = pl.BlockSpec(memory_space=pl.ANY)
    vmem = pl.BlockSpec(memory_space=pltpu.VMEM)
    dma = pltpu.SemaphoreType.DMA
    in_specs = [anywhere] * 19
    results = pl.pallas_call(
        kernel,
        out_shape=(
            pltpu.VMEM((ROWS, D), BF16),
            pltpu.VMEM((SEQS, KV), BF16),
            pltpu.VMEM((SEQS, ROPE), BF16),
        ),
        in_specs=in_specs,
        out_specs=(vmem, vmem, vmem),
        scratch_shapes=[
            pltpu.SMEM((SEQS,), I32),
            pltpu.VMEM((8, D), BF16),
            pltpu.VMEM((ROWS, SHARE), BF16),
            pltpu.VMEM((SEQS, LEN, KV), BF16),
            pltpu.VMEM((SEQS, ROPE, LEN), BF16),
            pltpu.VMEM((SEQS, H, KV), BF16),
            pltpu.VMEM((SEQS, H, ROPE), BF16),
            pltpu.VMEM((D,), BF16),
            pltpu.VMEM((D, KV), BF16),
            pltpu.VMEM((KV,), BF16),
            pltpu.VMEM((ROPE, D), BF16),
            pltpu.VMEM((KV, D), BF16),
            pltpu.VMEM((2, SHARE, HALF), BF16),
            pltpu.VMEM((D,), BF16),
            pltpu.VMEM((GROUPS, D), BF16),
            pltpu.VMEM((EXPERTS, D), BF16),
            pltpu.VMEM((2, ROWS), I32),
            pltpu.VMEM((2, D, HID), BF16),
            pltpu.VMEM((2, D, HID), BF16),
            pltpu.VMEM((2, HID, D), BF16),
            pltpu.VMEM((SEQS * H, KV), BF16),
            pltpu.VMEM((NZ, 8, SHARE), BF16),
            pltpu.VMEM((N_TP, 8, SHARE), BF16),
            pltpu.VMEM((NZ, ROWS, SHARE), F32),
            pltpu.VMEM((NZ, ROWS, SHARE), BF16),
            pltpu.VMEM((NZ, ROWS, SHARE), BF16),
            pltpu.VMEM((NZ, ROWS, SHARE), BF16),
            pltpu.VMEM((NZ, ROWS, SHARE), BF16),
            pltpu.VMEM((ROWS, D), BF16),
            pltpu.VMEM((SLOTS, ROWS), BF16),
            pltpu.VMEM((SLOTS, HALF), BF16),
            pltpu.VMEM((2, N_EP * CAP, HALF), BF16),
            pltpu.VMEM((2, N_EP * CAP, HALF), BF16),
            pltpu.VMEM((SLOTS, HALF), BF16),
            pltpu.VMEM((2 * ROWS, SLOTS), BF16),
            pltpu.VMEM((NZ, ROWS, SHARE), BF16),
            pltpu.VMEM((NZ, ROWS, SHARE), BF16),
            pltpu.VMEM((2, NZ, ROWS, SHARE), BF16),
            pltpu.VMEM((1, D), F32),
            pltpu.VMEM((SEQS, KV, LEN), BF16),
            pltpu.VMEM((2, H, LEN), F32),
            dma((21,)),
            dma((4,)),
            dma((4,)),
            dma,
            dma,
            dma,
            dma,
            dma,
            dma((len(OUT_GROUPS),)),
            dma,
            dma,
            dma((len(OUT_GROUPS),)),
            dma((len(OUT_GROUPS),)),
            dma((len(BACK_GROUPS),)),
            dma((len(BACK_GROUPS),)),
            dma,
            dma,
            dma,
            dma((NZ,)),
            dma,
            dma,
        ],
        compiler_params=pltpu.CompilerParams(
            collective_id=0, has_side_effects=True, vmem_limit_bytes=60 * 1024 * 1024
        ),
    )(
        residual,
        cache_latent,
        cache_rope,
        lengths,
        query_latent,
        query_rope,
        norm_gain,
        latent_weight,
        latent_gain,
        rope_weight,
        value_weight,
        out_weight,
        mixer_gain,
        group_router.T,
        expert_router.T,
        expert_ids.T,
        gate_weight,
        up_weight,
        down_weight,
    )
    return pl.pallas_call(
        write_out,
        out_shape=(
            jax.ShapeDtypeStruct((ROWS, D), BF16),
            jax.ShapeDtypeStruct((SEQS, KV), BF16),
            jax.ShapeDtypeStruct((SEQS, ROPE), BF16),
        ),
        in_specs=[vmem] * 3,
        out_specs=(anywhere,) * 3,
        scratch_shapes=[dma((3,))],
        compiler_params=pltpu.CompilerParams(vmem_limit_bytes=1024 * 1024),
    )(*results)


def solution(mesh):
    in_specs = (
        P("ep", None),
        P(("ep", "tp"), None, None),
        P(("ep", "tp"), None, None),
        P(("ep", "tp")),
        P(("ep", "tp"), None, None),
        P(("ep", "tp"), None, None),
        P(),
        P(),
        P(),
        P(),
        P(),
        P("tp", None),
        P(),
        P(),
        P(),
        P("ep", None),
        P("ep", None, "tp"),
        P("ep", None, "tp"),
        P("ep", "tp", None),
    )
    out_specs = (P("ep", None), P(("ep", "tp"), None), P(("ep", "tp"), None))
    return jax.shard_map(
        on_device, mesh=mesh, in_specs=in_specs, out_specs=out_specs, check_vma=False
    )
```

```python
import functools
import math

import jax
import jax.numpy as jnp
from jax import lax
from jax.experimental import pallas as pl
from jax.experimental.pallas import tpu as pltpu
from jax.sharding import PartitionSpec as P

MESH = pl.DeviceIdType.MESH
F32 = jnp.float32
BF16 = jnp.bfloat16
I32 = jnp.int32

D = 2048
HALF = D // 2
H = 32
KV = 256
ROPE = 32
NOPE = 64
V = 64
GROUPS = 4
LEN = 2048
CAP = 8
N_EP = 16
N_TP = 16
NZ = 8
SEQS = 4
ROWS = 64
EXPERTS = 32
SLOTS = EXPERTS * CAP
SHARE = 128
HID = 256
OTHERS = 2 * N_EP - 1
EPS = 1e-06
ROPE_BASE = 10000.0
ORDER = (4, 3, 5, 2, 6, 1, 7)
OUT_GROUPS = ((0,), (1, 7), (2, 6), (3, 5, 4))
BACK_GROUPS = ((4, 3, 5), (2, 6), (1, 7, 0))

FAR_FIRST = tuple(
    sorted(
        ((a, b) for a in range(4) for b in range(4) if a or b),
        key=lambda step: -sum(min(v, 4 - v) for v in step),
    )
)


def spans(groups):
    at, result = 0, []
    for group in groups:
        result.append((at * SHARE, len(group) * SHARE))
        at += len(group)
    return result


def dot(a, b):
    return jnp.dot(a, b, preferred_element_type=F32)


def dot_t(a, b):
    return lax.dot_general(a, b, (((1,), (1,)), ((), ())), preferred_element_type=F32)


def iota(shape, dim):
    return lax.broadcasted_iota(I32, shape, dim)


def kernel(
    residual,
    cache_latent,
    cache_rope,
    lengths_in,
    query_latent,
    query_rope,
    norm_gain,
    latent_weight,
    latent_gain,
    rope_weight,
    value_weight,
    out_weight,
    mixer_gain,
    group_router,
    expert_router,
    ids,
    gate_weight,
    up_weight,
    down_weight,
    mixed_out,
    new_latent_out,
    new_rope_out,
    lengths,
    res8,
    res_cols,
    cl,
    cr,
    ql,
    qr,
    ng,
    lw,
    lg,
    rw,
    vw,
    ow,
    mg,
    grt,
    ert,
    idv,
    gw,
    uw,
    dw,
    mixl,
    hv_send,
    hv_recv,
    acc,
    rs_send,
    rs_recv,
    after,
    after_other,
    full,
    sel,
    disp,
    xin,
    ret,
    yin,
    comb,
    rs2_send,
    rs2_recv,
    fin,
    gain2,
    lt,
    early,
    local_sem,
    w_ssem,
    w_rsem,
    hv_ssem,
    hv_rsem,
    rs_ssem,
    rs_rsem,
    ag_ssem,
    ag_rsem,
    ot_ssem,
    ot_rsem,
    x_ssem,
    x_rsem,
    y_ssem,
    y_rsem,
    rs2_ssem,
    rs2_rsem,
    f_ssem,
    f_rsem,
    p_ssem,
    p_rsem,
):
    ep = lax.axis_index("ep")
    tp = lax.axis_index("tp")
    z = lax.div(tp, 2)
    c = lax.rem(tp, 2)
    other = 1 - c
    partner = z * 2 + other

    def remote(src, dst, ssem, rsem, to_ep, to_tp):
        return pltpu.make_async_remote_copy(
            src_ref=src,
            dst_ref=dst,
            send_sem=ssem,
            recv_sem=rsem,
            device_id=(to_ep, to_tp),
            device_id_type=MESH,
        )

    def ring(i):
        return lax.rem(z + i, NZ)

    barrier = pltpu.get_barrier_semaphore()

    def signal_tp(i, carry):
        pl.semaphore_signal(
            barrier, inc=1, device_id=(ep, lax.rem(tp + i, N_TP)), device_id_type=MESH
        )
        return carry

    def signal_ep(i, carry):
        there = lax.rem(ep + i, N_EP)
        for core in range(2):
            pl.semaphore_signal(
                barrier, inc=1, device_id=(there, z * 2 + core), device_id_type=MESH
            )
        return carry

    loads = {}

    def load(name, src, dst):
        copy = pltpu.make_async_copy(src, dst, local_sem.at[len(loads)])
        copy.start()
        loads[name] = copy

    load("ql", query_latent, ql)
    load("cl0", cache_latent.at[0:2], cl.at[0:2])
    load("len", lengths_in, lengths)
    load("res8", residual.at[pl.ds(pl.multiple_of(z * 8, 8), 8), :], res8)
    load("ng", norm_gain, ng)
    load("lg", latent_gain, lg)
    load("rw", rope_weight, rw)
    load("qr", query_rope, qr)
    load("lw", latent_weight, lw)
    load("cr", cache_rope, cr)
    load("cl2", cache_latent.at[2:4], cl.at[2:4])

    lax.fori_loop(1, N_TP, signal_tp, 0)
    lax.fori_loop(1, N_EP, signal_ep, 0)

    loads["ql"].wait()
    loads["cl0"].wait()
    for s in range(2):
        lt[s] = cl[s].T
        early[s] = dot(ql[s], lt[s])

    for name in ("len", "res8", "ng", "lg", "rw", "qr", "lw", "cr", "cl2"):
        loads[name].wait()
    rows = res8[...].astype(F32)
    inv = lax.rsqrt(jnp.mean(rows * rows, axis=1, keepdims=True) + EPS)
    normed = (rows * inv * ng[...].astype(F32)[None, :]).astype(BF16)
    rope_raw = dot_t(normed, rw[...])
    latent_raw = dot(normed, lw[...])
    inv = lax.rsqrt(jnp.mean(latent_raw * latent_raw, axis=1, keepdims=True) + EPS)
    latent8 = latent_raw * inv * lg[...].astype(F32)[None, :]

    def own_rows(v):
        first = (iota(v.shape, 0) * 0 + c) == 0
        return jnp.where(first, v, pltpu.roll(v, 4, 0))

    new_latent = own_rows(latent8).astype(BF16)
    new_latent_out[...] = new_latent[0:SEQS]
    rope_own = own_rows(rope_raw)

    lane = iota((8, ROPE), 1)
    row = iota((8, ROPE), 0)
    place = lax.rem(lane, ROPE // 2).astype(F32)
    freq = jnp.exp(place * (-math.log(ROPE_BASE) / (ROPE // 2)))
    pos = jnp.zeros((8, ROPE), I32)
    for s in range(SEQS):
        pos = jnp.where(row == s, lengths[s], pos)
    angle = pos.astype(F32) * freq
    cos = jnp.cos(angle)
    sin = jnp.sin(angle)
    sin = jnp.where(lane < ROPE // 2, -sin, sin)

    def swapped(u):
        return jnp.concatenate([u[:, ROPE // 2 :], u[:, : ROPE // 2]], axis=1)

    new_rope = (rope_own * cos + swapped(rope_own) * sin).astype(BF16)
    new_rope_out[...] = new_rope[0:SEQS]
    new_latent_f = new_latent.astype(F32)
    new_rope_f = new_rope.astype(F32)

    scale = (NOPE + ROPE) ** (-0.5)
    def attend(s):
        u = qr[s].astype(F32)
        turned = (u * cos[s : s + 1] + swapped(u) * sin[s : s + 1]).astype(BF16)
        q = ql[s]
        latents = cl[s]
        if s < 2:
            score = early[s]
        else:
            lt[s] = latents.T
            score = dot(q, lt[s])
        score = (score + dot(turned, cr[s])) * scale
        keep = iota((H, LEN), 1) < lengths[s]
        score = jnp.where(keep, score, -jnp.inf)
        fresh = (
            jnp.sum(q.astype(F32) * new_latent_f[s : s + 1], axis=1, keepdims=True)
            + jnp.sum(turned.astype(F32) * new_rope_f[s : s + 1], axis=1, keepdims=True)
        ) * scale
        top = jnp.maximum(jnp.max(score, axis=1, keepdims=True), fresh)
        e = jnp.exp(score - top)
        fresh_e = jnp.exp(fresh - top)
        total = jnp.sum(e, axis=1, keepdims=True) + fresh_e
        weight = (e / total).astype(BF16)
        fresh_w = (fresh_e / total).astype(BF16).astype(F32)
        mixed = dot(weight, latents) + fresh_w * new_latent_f[s : s + 1]
        mixl[s * H : (s + 1) * H, :] = mixed.astype(BF16)

    load("vw", value_weight, vw)
    load("ow", out_weight.at[:, pl.ds(pl.multiple_of(c * HALF, HALF), HALF)], ow.at[c])
    share_at = pl.multiple_of(c * HALF + z * SHARE, SHARE)
    load("res_cols", residual.at[:, pl.ds(share_at, SHARE)], res_cols)
    load("ids", ids, idv)
    load("mg", mixer_gain, mg)
    load("grt", group_router, grt)
    load("ert", expert_router, ert)
    for s in range(SEQS):
        attend(s)
    pl.semaphore_wait(barrier, 45)
    swaps = [
        remote(
            out_weight.at[:, pl.ds(pl.multiple_of(other * HALF, HALF), HALF)],
            ow.at[c],
            w_ssem.at[0],
            w_rsem.at[0],
            ep,
            partner,
        ),
        remote(gate_weight.at[other], gw.at[1], w_ssem.at[1], w_rsem.at[1], ep, partner),
        remote(up_weight.at[other], uw.at[1], w_ssem.at[2], w_rsem.at[2], ep, partner),
        remote(down_weight.at[other], dw.at[1], w_ssem.at[3], w_rsem.at[3], ep, partner),
    ]
    swaps[0].start()

    loads["vw"].wait()
    wide = dot(mixl[...], vw[...])
    own = (iota((SEQS * H, D), 1) // V) == lax.rem(iota((SEQS * H, D), 0), H)
    wide = jnp.where(own, wide, 0.0).astype(BF16)
    pick = (iota((8, SEQS * H), 1) // H) == lax.rem(iota((8, SEQS * H), 0), SEQS)
    heads = dot(pick.astype(F32).astype(BF16), wide)
    low = iota((8, SHARE), 0) < SEQS
    for zz in range(NZ):
        a = heads[:, zz * 256 : zz * 256 + 128]
        b = heads[:, zz * 256 + 128 : zz * 256 + 256]
        hv_send[zz] = jnp.where(low, a, b).astype(BF16)

    def hv_copy(i):
        there = lax.rem(tp + i, N_TP)
        return remote(
            hv_send.at[lax.div(there, 2)], hv_recv.at[tp], hv_ssem, hv_rsem, ep, there
        )

    for i in (8, 7, 9, 6, 10, 5, 11, 4, 12, 3, 13, 2, 14, 1, 15):
        hv_copy(i).start()
    hv_recv[tp] = hv_send[z]
    swaps[1].start()
    swaps[2].start()
    load("gw", gate_weight.at[c], gw.at[0])
    load("uw", up_weight.at[c], uw.at[0])
    load("dw", down_weight.at[c], dw.at[0])

    loads["ids"].wait()
    idr = idv[...]
    e_row = [idr[k : k + 1, :] for k in range(2)]
    eye = iota((ROWS, ROWS), 0) == iota((ROWS, ROWS), 1)

    def to_col(v):
        return jnp.sum(jnp.where(eye, jnp.broadcast_to(v, (ROWS, ROWS)), 0.0), axis=1, keepdims=True)

    def to_row(v):
        return jnp.sum(jnp.where(eye, jnp.broadcast_to(v, (ROWS, ROWS)), 0.0), axis=0, keepdims=True)

    e_col = [to_col(v.astype(F32)) for v in e_row]
    expert_iota = iota((ROWS, EXPERTS), 1).astype(F32)
    hits = [(jnp.broadcast_to(v, (ROWS, EXPERTS)) == expert_iota).astype(F32) for v in e_col]
    before = (iota((ROWS, ROWS), 1) < iota((ROWS, ROWS), 0)).astype(F32).astype(BF16)
    counts = dot(before, (hits[0] + hits[1]).astype(BF16))
    slot_col = [
        e_col[k] * CAP + jnp.sum(counts * hits[k], axis=1, keepdims=True) for k in range(2)
    ]
    slot_iota = iota((SLOTS, ROWS), 0).astype(F32)
    chosen = jnp.zeros((SLOTS, ROWS), F32)
    for k in range(2):
        chosen += (jnp.broadcast_to(to_row(slot_col[k]), (SLOTS, ROWS)) == slot_iota).astype(F32)
    sel[...] = chosen.astype(BF16)

    all_heads = hv_recv.at[0 : N_TP - 1]
    remote(all_heads, all_heads, hv_ssem, hv_rsem, ep, partner).wait_recv()

    loads["ow"].wait()
    swaps[0].wait_recv()
    heads_in = hv_recv[...].astype(F32).reshape(N_TP * 8, SHARE).astype(BF16)
    part = None
    for k in range(2):
        r = iota((ROWS, N_TP * 8), 0)
        j = iota((ROWS, N_TP * 8), 1)
        rows_k = (j == 8 * (r // SEQS) + SEQS * k + lax.rem(r, SEQS)).astype(F32).astype(BF16)
        term = dot(dot(rows_k, heads_in).astype(BF16), ow[k])
        part = term if part is None else part + term
    for zz in range(NZ):
        acc[zz] = part[:, zz * SHARE : (zz + 1) * SHARE]
    for i in ORDER:
        rs_send[i] = acc[ring(i)].astype(BF16)

    def scatter_copy(send, recv, ssem, rsem, i):
        return remote(send.at[i], recv.at[z], ssem, rsem, ep, ring(i) * 2 + c)

    def scatter(send, recv, ssem, rsem, steps):
        for i in steps:
            scatter_copy(send, recv, ssem, rsem, i).start()

    def scatter_all(recv, ssem, rsem):
        seven = recv.at[0 : NZ - 1]
        return remote(seven, seven, ssem, rsem, ep, partner)

    def scatter_wait(recv, ssem, rsem, total):
        scatter_all(recv, ssem, rsem).wait_recv()
        for i in ORDER:
            total += recv[ring(i)].astype(F32)
        return total

    scatter(rs_send, rs_recv, rs_ssem, rs_rsem, ORDER)
    swaps[3].start()
    loads["res_cols"].wait()
    total = res_cols[...].astype(F32) + scatter_wait(rs_recv, rs_ssem, rs_rsem, acc[z])
    after[z] = total.astype(BF16)

    def group_of(i):
        return [i in group for group in OUT_GROUPS].index(True)

    def ag_copy(i):
        return remote(
            after.at[z], after.at[z], ag_ssem, ag_rsem.at[group_of(NZ - i)], ep, ring(i) * 2 + c
        )

    for i in reversed(ORDER):
        ag_copy(i).start()

    mine = pl.ds(pl.multiple_of((ep * 2 + c) * CAP, CAP), CAP)
    here = pl.ds(pl.multiple_of(ep * CAP, CAP), CAP)
    theirs = pl.ds(pl.multiple_of((ep * 2 + other) * CAP, CAP), CAP)

    def away(step):
        down, right = step
        return lax.rem(lax.div(ep, 4) + down, 4) * 4 + lax.rem(ep + right, 4)

    def x_copy(n, step, core):
        there = away(step)
        at = pl.ds(pl.multiple_of((there * 2 + core) * CAP, CAP), CAP)
        cols = pl.ds(*spans(OUT_GROUPS)[n])
        return remote(
            disp.at[at, cols],
            xin.at[c, here, cols],
            x_ssem.at[n],
            x_rsem.at[n],
            there,
            z * 2 + core,
        )

    for n, group in enumerate(OUT_GROUPS):
        base = spans(OUT_GROUPS)[n][0]
        come = after.at[0 : max(1, len(group) - (0 in group))]
        if group != (0,):
            remote(come, come, ag_ssem, ag_rsem.at[n], ep, partner).wait_recv()
        for place_at, i in enumerate(group):
            at = base + place_at * SHARE
            disp[:, at : at + SHARE] = dot(sel[...], after[ring(i)]).astype(BF16)
        for step in FAR_FIRST:
            for core in range(2):
                x_copy(n, step, core).start()
        x_copy(n, (0, 0), other).start()
    xin[c, here, :] = disp[mine, :]
    to_partner = remote(after, after_other, ot_ssem, ot_rsem, ep, partner)
    to_partner.start()

    loads["mg"].wait()
    loads["grt"].wait()
    loads["ert"].wait()
    to_partner.wait_recv()
    for zz in range(NZ):
        at = pl.ds(pl.multiple_of(c * HALF + zz * SHARE, SHARE), SHARE)
        full[:, at] = after[zz]
        at = pl.ds(pl.multiple_of(other * HALF + zz * SHARE, SHARE), SHARE)
        full[:, at] = after_other[zz]
    gain = mg[...].astype(F32)[None, :]
    gain2[...] = gain
    rows = full[...].astype(F32)
    inv = lax.rsqrt(jnp.mean(rows * rows, axis=1, keepdims=True) + EPS)
    expert_in = (rows * inv * gain).astype(BF16)
    group_logits = dot_t(expert_in, grt[...])
    expert_logits = dot_t(expert_in, ert[...])
    group_of = jnp.floor(e_col[0] * (GROUPS / EXPERTS))
    group_hit = jnp.broadcast_to(group_of, (ROWS, GROUPS)) == iota((ROWS, GROUPS), 1).astype(F32)
    group_pick = jnp.sum(jnp.where(group_hit, group_logits, 0.0), axis=1, keepdims=True)
    share = 1.0 / jnp.sum(jnp.exp(group_logits - group_pick), axis=1, keepdims=True)
    picked = [jnp.sum(hits[k] * expert_logits, axis=1, keepdims=True) for k in range(2)]
    weights = jnp.zeros((ROWS, SLOTS), F32)
    wide_iota = iota((ROWS, SLOTS), 1).astype(F32)
    for k in range(2):
        inner = 1.0 / (1.0 + jnp.exp(picked[1 - k] - picked[k]))
        weights += jnp.where(
            jnp.broadcast_to(slot_col[k], (ROWS, SLOTS)) == wide_iota, share * inner, 0.0
        )
    high = weights.astype(BF16)
    comb[0:ROWS, :] = high
    comb[ROWS:, :] = (weights - high.astype(F32)).astype(BF16)

    sent = pl.ds(0, OTHERS * CAP)

    def x_all(n):
        part_of = disp.at[sent, pl.ds(*spans(OUT_GROUPS)[n])]
        return remote(part_of, part_of, x_ssem.at[n], x_rsem.at[n], ep, partner)

    def y_all(n):
        part_of = yin.at[sent, pl.ds(*spans(BACK_GROUPS)[n])]
        return remote(part_of, part_of, y_ssem.at[n], y_rsem.at[n], ep, partner)

    for name in ("gw", "uw"):
        loads[name].wait()
    swaps[1].wait_recv()
    swaps[2].wait_recv()
    products = [0.0, 0.0, 0.0, 0.0]
    square = 0.0
    for n, group in enumerate(OUT_GROUPS):
        x_all(n).wait_recv()
        base = spans(OUT_GROUPS)[n][0]
        for core in range(2):
            for place_at, i in enumerate(group):
                at = pl.ds(pl.multiple_of(core * HALF + ring(i) * SHARE, SHARE), SHARE)
                to = base + place_at * SHARE
                piece = xin[core, :, to : to + SHARE].astype(F32)
                square += piece * piece
                scaled = (piece * gain2[:, at]).astype(BF16)
                for k in range(2):
                    products[k] += dot(scaled, gw[k, at, :])
                    products[2 + k] += dot(scaled, uw[k, at, :])
    inv = lax.rsqrt(jnp.sum(square, axis=1, keepdims=True) * (1.0 / D) + EPS)
    acts = []
    for k in range(2):
        g = products[k] * inv
        u = products[2 + k] * inv
        acts.append((g * (1.0 / (1.0 + jnp.exp(-g))) * u).astype(BF16))
    loads["dw"].wait()
    swaps[3].wait_recv()

    def y_copy(n, step, half):
        there = away(step)
        at = pl.ds(pl.multiple_of(there * CAP, CAP), CAP)
        cols = pl.ds(*spans(BACK_GROUPS)[n])
        return remote(
            ret.at[half, at, cols],
            yin.at[mine, cols],
            y_ssem.at[n],
            y_rsem.at[n],
            there,
            z * 2 + half,
        )

    for n, group in enumerate(BACK_GROUPS):
        base = spans(BACK_GROUPS)[n][0]
        for half in range(2):
            for place_at, i in enumerate(group):
                at = pl.ds(pl.multiple_of(half * HALF + ring(i) * SHARE, SHARE), SHARE)
                to = base + place_at * SHARE
                ret[half, :, to : to + SHARE] = (
                    dot(acts[0], dw[0, :, at]) + dot(acts[1], dw[1, :, at])
                ).astype(BF16)

        for step in FAR_FIRST:
            for half in range(2):
                y_copy(n, step, half).start()
        y_copy(n, (0, 0), other).start()
    yin[mine, :] = ret[c, here, :]

    for n, group in enumerate(BACK_GROUPS):
        y_all(n).wait_recv()
        base, width = spans(BACK_GROUPS)[n]
        both = dot(comb[...], yin[:, base : base + width])
        moe = both[0:ROWS] + both[ROWS:]
        for place_at, i in enumerate(group):
            piece = moe[:, place_at * SHARE : (place_at + 1) * SHARE]
            if i:
                rs2_send[i] = piece.astype(BF16)
                scatter(rs2_send, rs2_recv, rs2_ssem, rs2_rsem, (i,))
            else:
                acc[0] = piece
    total = after[z].astype(F32) + scatter_wait(rs2_recv, rs2_ssem, rs2_rsem, acc[0])
    fin[c, z] = total.astype(BF16)

    def f_copy(i):
        return remote(
            fin.at[c, z], fin.at[c, z], f_ssem, f_rsem.at[z], ep, ring(i) * 2 + c
        )

    def p_copy(zz):
        return remote(fin.at[c, zz], fin.at[c, zz], p_ssem, p_rsem, ep, partner)

    for i in ORDER:
        f_copy(i).start()
    p_copy(z).start()
    for i in reversed(ORDER):
        src = ring(i)
        remote(
            fin.at[c, src], fin.at[c, src], f_ssem, f_rsem.at[src], ep, src * 2 + c
        ).wait_recv()
        p_copy(src).start()

    def spread(core, zz):
        at = pl.ds(pl.multiple_of(core * HALF + zz * SHARE, SHARE), SHARE)
        mixed_out[:, at] = fin[core, zz]

    for zz in range(NZ):
        spread(c, zz)
    remote(fin.at[other], fin.at[other], p_ssem, p_rsem, ep, partner).wait_recv()
    for zz in range(NZ):
        spread(other, zz)

    for copy in swaps:
        copy.wait_send()
    remote(all_heads, all_heads, hv_ssem, hv_rsem, ep, partner).wait_send()
    scatter_all(rs_recv, rs_ssem, rs_rsem).wait_send()
    scatter_all(rs2_recv, rs2_ssem, rs2_rsem).wait_send()
    scatter_all(after, ag_ssem, rs_rsem).wait_send()
    scatter_all(rs_recv, f_ssem, rs_rsem).wait_send()
    remote(fin.at[other], fin.at[other], p_ssem, p_rsem, ep, partner).wait_send()
    to_partner.wait_send()
    for n in range(len(OUT_GROUPS)):
        x_all(n).wait_send()
    for n in range(len(BACK_GROUPS)):
        y_all(n).wait_send()


def write_out(a, b, c, a_out, b_out, c_out, sem):
    copies = [
        pltpu.make_async_copy(src, dst, sem.at[i])
        for i, (src, dst) in enumerate(((a, a_out), (b, b_out), (c, c_out)))
    ]
    for copy in copies:
        copy.start()
    for copy in copies:
        copy.wait()


def on_device(
    residual,
    cache_latent,
    cache_rope,
    lengths,
    query_latent,
    query_rope,
    norm_gain,
    latent_weight,
    latent_gain,
    rope_weight,
    value_weight,
    out_weight,
    mixer_gain,
    group_router,
    expert_router,
    expert_ids,
    gate_weight,
    up_weight,
    down_weight,
):
    anywhere = pl.BlockSpec(memory_space=pl.ANY)
    vmem = pl.BlockSpec(memory_space=pltpu.VMEM)
    dma = pltpu.SemaphoreType.DMA
    in_specs = [anywhere] * 19
    results = pl.pallas_call(
        kernel,
        out_shape=(
            pltpu.VMEM((ROWS, D), BF16),
            pltpu.VMEM((SEQS, KV), BF16),
            pltpu.VMEM((SEQS, ROPE), BF16),
        ),
        in_specs=in_specs,
        out_specs=(vmem, vmem, vmem),
        scratch_shapes=[
            pltpu.SMEM((SEQS,), I32),
            pltpu.VMEM((8, D), BF16),
            pltpu.VMEM((ROWS, SHARE), BF16),
            pltpu.VMEM((SEQS, LEN, KV), BF16),
            pltpu.VMEM((SEQS, ROPE, LEN), BF16),
            pltpu.VMEM((SEQS, H, KV), BF16),
            pltpu.VMEM((SEQS, H, ROPE), BF16),
            pltpu.VMEM((D,), BF16),
            pltpu.VMEM((D, KV), BF16),
            pltpu.VMEM((KV,), BF16),
            pltpu.VMEM((ROPE, D), BF16),
            pltpu.VMEM((KV, D), BF16),
            pltpu.VMEM((2, SHARE, HALF), BF16),
            pltpu.VMEM((D,), BF16),
            pltpu.VMEM((GROUPS, D), BF16),
            pltpu.VMEM((EXPERTS, D), BF16),
            pltpu.VMEM((2, ROWS), I32),
            pltpu.VMEM((2, D, HID), BF16),
            pltpu.VMEM((2, D, HID), BF16),
            pltpu.VMEM((2, HID, D), BF16),
            pltpu.VMEM((SEQS * H, KV), BF16),
            pltpu.VMEM((NZ, 8, SHARE), BF16),
            pltpu.VMEM((N_TP, 8, SHARE), BF16),
            pltpu.VMEM((NZ, ROWS, SHARE), F32),
            pltpu.VMEM((NZ, ROWS, SHARE), BF16),
            pltpu.VMEM((NZ, ROWS, SHARE), BF16),
            pltpu.VMEM((NZ, ROWS, SHARE), BF16),
            pltpu.VMEM((NZ, ROWS, SHARE), BF16),
            pltpu.VMEM((ROWS, D), BF16),
            pltpu.VMEM((SLOTS, ROWS), BF16),
            pltpu.VMEM((SLOTS, HALF), BF16),
            pltpu.VMEM((2, N_EP * CAP, HALF), BF16),
            pltpu.VMEM((2, N_EP * CAP, HALF), BF16),
            pltpu.VMEM((SLOTS, HALF), BF16),
            pltpu.VMEM((2 * ROWS, SLOTS), BF16),
            pltpu.VMEM((NZ, ROWS, SHARE), BF16),
            pltpu.VMEM((NZ, ROWS, SHARE), BF16),
            pltpu.VMEM((2, NZ, ROWS, SHARE), BF16),
            pltpu.VMEM((1, D), F32),
            pltpu.VMEM((SEQS, KV, LEN), BF16),
            pltpu.VMEM((2, H, LEN), F32),
            dma((21,)),
            dma((4,)),
            dma((4,)),
            dma,
            dma,
            dma,
            dma,
            dma,
            dma((len(OUT_GROUPS),)),
            dma,
            dma,
            dma((len(OUT_GROUPS),)),
            dma((len(OUT_GROUPS),)),
            dma((len(BACK_GROUPS),)),
            dma((len(BACK_GROUPS),)),
            dma,
            dma,
            dma,
            dma((NZ,)),
            dma,
            dma,
        ],
        compiler_params=pltpu.CompilerParams(
            collective_id=0, has_side_effects=True, vmem_limit_bytes=60 * 1024 * 1024
        ),
    )(
        residual,
        cache_latent,
        cache_rope,
        lengths,
        query_latent,
        query_rope,
        norm_gain,
        latent_weight,
        latent_gain,
        rope_weight,
        value_weight,
        out_weight,
        mixer_gain,
        group_router.T,
        expert_router.T,
        expert_ids.T,
        gate_weight,
        up_weight,
        down_weight,
    )
    return pl.pallas_call(
        write_out,
        out_shape=(
            jax.ShapeDtypeStruct((ROWS, D), BF16),
            jax.ShapeDtypeStruct((SEQS, KV), BF16),
            jax.ShapeDtypeStruct((SEQS, ROPE), BF16),
        ),
        in_specs=[vmem] * 3,
        out_specs=(anywhere,) * 3,
        scratch_shapes=[dma((3,))],
        compiler_params=pltpu.CompilerParams(vmem_limit_bytes=1024 * 1024),
    )(*results)


def solution(mesh):
    in_specs = (
        P("ep", None),
        P(("ep", "tp"), None, None),
        P(("ep", "tp"), None, None),
        P(("ep", "tp")),
        P(("ep", "tp"), None, None),
        P(("ep", "tp"), None, None),
        P(),
        P(),
        P(),
        P(),
        P(),
        P("tp", None),
        P(),
        P(),
        P(),
        P("ep", None),
        P("ep", None, "tp"),
        P("ep", None, "tp"),
        P("ep", "tp", None),
    )
    out_specs = (P("ep", None), P(("ep", "tp"), None), P(("ep", "tp"), None))
    return jax.shard_map(
        on_device, mesh=mesh, in_specs=in_specs, out_specs=out_specs, check_vma=False
    )
```
